512 devices in a mesh: grp: 2 (over y), sp: 32 (over z), tp: 8 (over x, core).
Axes of the slice: x: 4, y: 2, z: 32, core: 2. Of those that a mesh axis runs over, the one named last changes fastest.
The devices are a block of a 4x8x32 slice.
Arguments:
- tokens: bfloat16 [8192, 2048], P(('grp', 'sp')), parts along dimension 0, may hold values from -8 to 8
- norm_gain: float32 [2048], replicated, may hold values from 0.1 to 1.9
- w_query: bfloat16 [2048, 1024], P(None, 'tp'), may hold values from -0.125 to 0.125
- w_key: bfloat16 [2048, 1024], P(None, 'tp'), may hold values from -0.125 to 0.125
- w_value: bfloat16 [2048, 1024], P(None, 'tp'), may hold values from -0.125 to 0.125
- w_out: bfloat16 [1024, 2048], P('tp'), may hold values from -0.1875 to 0.1875
- key_rate: bfloat16 [16, 8192], P('tp', ('grp', 'sp')), parts along dimension 1, may hold values from -16 to 1
Outputs:
- layer_out: bfloat16 [8192, 2048], P(('grp', 'sp')), parts along dimension 0
The draws below stay inside these ranges and needn't reach their ends.
There are 2 independent parts, one for each index of `grp`. The reference program is written for one: setup_inputs(seed, part) draws one part's arguments, and reference() takes and returns one part's arrays. A program takes and returns all parts, laid end to end along the dimension named above; an argument that names none is the same for every part. Nothing has to cross between parts.
All inputs are finite; a program needn't handle non-finite values.
Results may differ from the reference program's by a relative error of at most 0.0075.
Values may be sent and summed in bfloat16 or wider, within the bound.
A program may use at most 64 MiB of HBM per device.

```python
import jax
import jax.numpy as jnp
from jax import lax

D = 2048
HEAD_TOTAL = 16
HD = 64
KEY_SPAN = 128
TOK_DEV = 128
TOKEN_TOTAL = 4096


def draw_tokens(key, part):
    noise_key, offset_key = jax.random.split(jax.random.fold_in(key, 3))
    block_count = TOKEN_TOTAL // TOK_DEV
    base_draw = jax.random.normal(noise_key, (TOKEN_TOTAL, D), jnp.float32)
    offsets = 0.8 * jax.random.normal(offset_key, (block_count, D), jnp.float32)
    drawn_rows = base_draw + jnp.repeat(offsets, TOK_DEV, axis=0)
    return jnp.clip(drawn_rows, -8.0, 8.0).astype(jnp.bfloat16)


def draw_key_rate(key, part):
    random_subkeys = jax.random.split(jax.random.fold_in(key, 7), 7)
    block_count = TOKEN_TOTAL // TOK_DEV
    slow_share = 0.5
    slow_heads = jax.random.uniform(random_subkeys[0], (HEAD_TOTAL,), jnp.float32) < slow_share
    log_length = jnp.log(jnp.float32(TOKEN_TOTAL))
    slow_rate = -log_length + jax.random.uniform(random_subkeys[1], (HEAD_TOTAL,), jnp.float32, -1.0, 0.3)
    fast_rate = jax.random.uniform(random_subkeys[2], (HEAD_TOTAL,), jnp.float32, -4.5, -3.0)
    head_rate = jnp.where(slow_heads, slow_rate, fast_rate)
    block_term = jax.random.uniform(random_subkeys[3], (HEAD_TOTAL, block_count), jnp.float32, -0.7, 0.7)
    rough = 0.3 * jax.random.normal(random_subkeys[4], (HEAD_TOTAL, TOKEN_TOTAL), jnp.float32)
    spike_position = jax.random.randint(random_subkeys[5], (4,), 0, TOKEN_TOTAL)
    spike_level = jax.random.uniform(random_subkeys[6], (HEAD_TOTAL, 4), jnp.float32, -1.5, 0.0)
    token_positions = jnp.arange(TOKEN_TOTAL, dtype=jnp.int32)
    match_count = token_positions[None, :] == spike_position[:, None]
    spike_value = jnp.einsum('me,eq->mq', spike_level, match_count.astype(jnp.float32))
    spike_flag = jnp.any(match_count, axis=0)
    rate_row_values = head_rate[:, None] + jnp.repeat(block_term, TOK_DEV, axis=1) + rough
    rate_row_values = jnp.where(spike_flag[None, :], spike_value, rate_row_values)
    return jnp.clip(rate_row_values, -16.0, 1.0).astype(jnp.bfloat16)


def levels(own_key, dims, cuts, low, high):
    gain = 1.0
    for axis_at, shards_of in cuts:
        heights = jax.random.uniform(jax.random.fold_in(jax.random.fold_in(own_key, 6), axis_at), (shards_of,), jnp.float32, low / len(cuts), high / len(cuts))
        gain = gain * jnp.repeat(jnp.exp(heights), dims[axis_at] // shards_of).reshape((-1,) + (1,) * (len(dims) - 1 - axis_at))
    return gain


def centred(rng, extent, spread, limit, pieces=(), kind=jnp.bfloat16):
    level = levels(rng, extent, pieces, -0.22, 0.18) if pieces else 1.0
    array = jax.random.normal(rng, extent, jnp.float32) * spread * level
    return jnp.minimum(jnp.maximum(array, -limit), limit).astype(kind)


def setup_inputs(seed: int = 0, part: int = 0) -> dict:
    key_list = jax.random.split(jax.random.key(seed), 8)
    own_keys = jax.random.split(jax.random.fold_in(key_list[7], part), 8)
    return {
        "tokens": draw_tokens(jax.random.fold_in(jax.random.fold_in(key_list[7], part), 71), part),
        "norm_gain": jnp.clip(1.0 + 0.18 * jax.random.normal(key_list[1], (D,), jnp.float32), 0.1, 1.9),
        "w_query": centred(key_list[2], (D, HEAD_TOTAL * HD), D ** -0.5, 0.125, ((1, 8),)),
        "w_key": centred(key_list[3], (D, HEAD_TOTAL * HD), D ** -0.5, 0.125, ((1, 8),)),
        "w_value": centred(key_list[4], (D, HEAD_TOTAL * HD), D ** -0.5, 0.125, ((1, 8),)),
        "w_out": centred(key_list[5], (HEAD_TOTAL * HD, D), (HEAD_TOTAL * HD) ** -0.5, 0.1875, ((0, 8),)),
        "key_rate": draw_key_rate(jax.random.fold_in(jax.random.fold_in(key_list[7], part), 71), part),
    }


F32 = jnp.float32
BF16 = jnp.bfloat16
HIGHEST = lax.Precision.HIGHEST
EPS = 1e-06

def shard_summary(query_heads, key_heads, value_heads, rate_row_values, query_pos, key_pos):
    scores = jnp.einsum('qhd,khd->hqk', query_heads.astype(F32), key_heads.astype(F32)) * HD ** (-0.5)
    scores = scores + jnp.transpose(rate_row_values).astype(F32)[:, None, :]
    causal_mask = key_pos[None, :] < query_pos[:, None]
    log_remain = jnp.where(causal_mask[None], jax.nn.log_sigmoid(-scores), 0.0)
    heads_here, query_count, key_count = scores.shape
    span_count = key_count // KEY_SPAN
    blocks = log_remain.reshape(heads_here, query_count, span_count, KEY_SPAN)
    span_ids = jnp.arange(KEY_SPAN, dtype=jnp.int32)
    tri_strict = (span_ids[:, None] > span_ids[None, :]).astype(F32)
    inside_sum = jnp.einsum('hqnj,js->hqns', blocks, tri_strict, precision=HIGHEST)
    block_ids = jnp.arange(span_count, dtype=jnp.int32)
    block_later = (block_ids[:, None] > block_ids[None, :]).astype(F32)
    beyond = jnp.einsum('hqn,nm->hqm', lax.optimization_barrier(jnp.sum(blocks, axis=-1)), block_later, precision=HIGHEST)
    suffix = (inside_sum + beyond[..., None]).reshape(heads_here, query_count, key_count)
    weight = jnp.where(causal_mask[None], jnp.exp(jax.nn.log_sigmoid(scores) + suffix), 0.0).astype(BF16)
    weight = lax.optimization_barrier(weight).astype(F32)
    partial_value = jnp.einsum('hqk,khd->qhd', weight, value_heads.astype(F32))
    return (partial_value.reshape(query_count, heads_here * HD), lax.optimization_barrier(jnp.sum(log_remain, axis=-1)))

def reference(tokens, norm_gain, w_query, w_key, w_value, w_out, key_rate):
    tokens_f = tokens.astype(F32)
    normed = (tokens_f * lax.rsqrt(lax.optimization_barrier(jnp.mean(tokens_f * tokens_f, axis=-1, keepdims=True)) + EPS) * norm_gain).astype(BF16)
    queries = lax.optimization_barrier(jnp.dot(normed, w_query, preferred_element_type=F32).astype(BF16))
    key_rows = lax.optimization_barrier(jnp.dot(normed, w_key, preferred_element_type=F32).astype(BF16))
    value_rows = lax.optimization_barrier(jnp.dot(normed, w_value, preferred_element_type=F32).astype(BF16))
    shard_total = TOKEN_TOTAL // TOK_DEV
    query_shards = queries.reshape(shard_total, TOK_DEV, HEAD_TOTAL, HD)
    key_shards = key_rows.reshape(shard_total, TOK_DEV, HEAD_TOTAL, HD)
    value_shards = value_rows.reshape(shard_total, TOK_DEV, HEAD_TOTAL, HD)
    rate_shards = jnp.transpose(key_rate).reshape(shard_total, TOK_DEV, HEAD_TOTAL)
    local_pos = jnp.arange(TOK_DEV, dtype=jnp.int32)
    shard_ids = jnp.arange(shard_total, dtype=jnp.int32)
    later_mask = (shard_ids[:, None] > shard_ids[None, :]).astype(F32)

    def one_shard(item_tuple):
        query_index, query_heads = item_tuple
        query_pos = query_index * TOK_DEV + local_pos

        def absorb_one(state_pair, key_tuple):
            key_index, key_heads, value_heads, rate_row_values = key_tuple
            empty_pair = (jnp.zeros((TOK_DEV, HEAD_TOTAL * HD), F32), jnp.zeros((HEAD_TOTAL, TOK_DEV), F32))
            result = lax.cond(key_index <= query_index, lambda: shard_summary(query_heads, key_heads, value_heads, rate_row_values, query_pos, key_index * TOK_DEV + local_pos), lambda: empty_pair)
            return (state_pair, result)
        _, (partials, remains) = lax.scan(absorb_one, None, (shard_ids, key_shards, value_shards, rate_shards))
        beyond = jnp.einsum('nhq,nm->mhq', remains, later_mask, precision=HIGHEST)
        factor = jnp.transpose(jnp.exp(beyond), (0, 2, 1))[..., None]
        mixed_rows = lax.optimization_barrier(jnp.sum(partials.reshape(shard_total, TOK_DEV, HEAD_TOTAL, HD) * factor, axis=0))
        return mixed_rows.reshape(TOK_DEV, HEAD_TOTAL * HD).astype(BF16)
    mixed = lax.map(one_shard, (shard_ids, query_shards)).reshape(TOKEN_TOTAL, HEAD_TOTAL * HD)
    return jnp.dot(mixed, w_out, preferred_element_type=F32).astype(BF16)
```

```python
import functools

import jax
import jax.numpy as jnp
from jax import lax
from jax.experimental import pallas as pl
from jax.experimental.pallas import tpu as pltpu
from jax.sharding import PartitionSpec as P

HD = 64
SPAN = 128
PAD = 16

F32 = jnp.float32
BF16 = jnp.bfloat16
EPS = 1e-06
MESH = pl.DeviceIdType.MESH


def dot(a, b):
    return lax.dot_general(a, b, (((1,), (0,)), ((), ())), preferred_element_type=F32)


def dot_t(a, b):
    return lax.dot_general(a, b, (((1,), (1,)), ((), ())), preferred_element_type=F32)


def layer(
    nsp,
    ntp,
    far,
    tokens,
    gain,
    w_query,
    w_key,
    w_value,
    w_out,
    rate,
    out,
    kv,
    normed,
    other_tokens,
    queries,
    first_queries,
    far_sent,
    far_in,
    far_queries,
    far_back,
    far_got,
    tri,
    rate_now,
    late_rate,
    acc,
    past,
    mixed,
    first_mixed,
    w_all,
    total,
    late_sem,
    kv_send,
    kv_recv,
    w_send,
    w_recv,
    mx_send,
    mx_recv,
    tok_send,
    tok_recv,
    lr_send,
    lr_recv,
    fq_send,
    fq_recv,
    fa_send,
    fa_recv,
):
    z = lax.axis_index("sp")
    t = lax.axis_index("tp")
    chips = ntp // 2
    x, core = t // 2, lax.rem(t, 2)
    sibling = 2 * x + 1 - core
    reach = nsp - 1 - far
    lead = t == 0
    first = z == 0
    last = z == nsp - 1
    outset = jnp.logical_and(first, lead)
    deputy = jnp.logical_and(z == 1, lead)
    helper = jnp.logical_and(first, t == 1)
    host = jnp.logical_and(z >= 1, z <= reach)
    guest = z > far

    bar = pltpu.get_barrier_semaphore()

    def at(zz, tt):
        return {"sp": zz, "tp": tt}

    def greet(zz, tt):
        pl.semaphore_signal(bar, inc=1, device_id=at(zz, tt), device_id_type=MESH)

    def send(src, dst, ss, rs, zz, tt):
        return pltpu.make_async_remote_copy(
            src_ref=src, dst_ref=dst, send_sem=ss, recv_sem=rs, device_id=at(zz, tt), device_id_type=MESH
        )

    @pl.when(z >= 1)
    def _():
        greet(z - 1, t)

    for p in range(ntp):

        @pl.when(jnp.logical_and(t != 0, t != p))
        def _():
            greet(z, p)

    @pl.when(host)
    def _():
        greet(z + far, t)

    @pl.when(jnp.logical_and(jnp.logical_and(host, lead), z >= 2))
    def _():
        greet(0, 0)

    @pl.when(jnp.logical_and(first, t != 0))
    def _():
        greet(1, 0)

    @pl.when(deputy)
    def _():
        greet(0, 1)

    one = lambda flag: jnp.where(flag, 1, 0)
    expected = (
        one(jnp.logical_not(last))
        + jnp.where(lead, ntp - 1, ntp - 2)
        + one(guest)
        + one(outset) * (reach - 1)
        + one(deputy) * (ntp - 1)
        + one(helper)
    )

    row = lax.broadcasted_iota(jnp.int32, (2 * SPAN, 2 * SPAN), 0)
    col = lax.broadcasted_iota(jnp.int32, (2 * SPAN, 2 * SPAN), 1)
    later = jnp.logical_or(col >= SPAN, lax.rem(row, SPAN) >= col)
    tri[...] = jnp.where(later, 1.0, 0.0).astype(BF16)

    def split_heads(dst, q):
        lane = lax.broadcasted_iota(jnp.int32, (SPAN, 2 * HD), 1)
        qf = q.astype(F32)
        dst[:SPAN] = jnp.where(lane < HD, qf, 0.0).astype(BF16)
        dst[SPAN:] = jnp.where(lane >= HD, qf, 0.0).astype(BF16)

    def join_heads(a):
        lane = lax.broadcasted_iota(jnp.int32, (SPAN, 2 * HD), 1)
        return jnp.where(lane < HD, a[:SPAN], a[SPAN:])

    def project(src, slot):
        xs = src[...].astype(F32)
        scale = lax.rsqrt(jnp.mean(xs * xs, axis=-1, keepdims=True) + EPS)
        normed[...] = (xs * scale * gain[...]).astype(BF16)
        kv[slot, pl.ds(0, SPAN)] = dot(normed[...], w_key[...]).astype(BF16)
        kv[slot, pl.ds(SPAN, SPAN)] = dot(normed[...], w_value[...]).astype(BF16)
        kv[slot, pl.ds(2 * SPAN, PAD)] = jnp.concatenate(
            [rate[...].astype(F32), jnp.zeros((PAD - 2, SPAN), F32)], axis=0
        ).astype(BF16)
        return dot(normed[...], w_query[...]).astype(BF16) * HD ** (-0.5)

    def attend(q_ref, slot, diagonal):
        s = dot_t(q_ref[...], kv[slot, pl.ds(0, SPAN)])
        s = jnp.concatenate([s[:SPAN] + rate_now[0:1], s[SPAN:] + rate_now[1:2]], axis=0)
        soft = jnp.maximum(s, 0.0) + jnp.log(1.0 + jnp.exp(-jnp.abs(s)))
        if diagonal:
            r = lax.rem(lax.broadcasted_iota(jnp.int32, (2 * SPAN, SPAN), 0), SPAN)
            c = lax.broadcasted_iota(jnp.int32, (2 * SPAN, SPAN), 1)
            seen = c < r
            soft = jnp.where(seen, soft, 0.0)
        high = soft.astype(BF16)
        low = (soft - high.astype(F32)).astype(BF16)
        sums = dot(jnp.concatenate([high, low], axis=1), tri[...])
        weight = jnp.exp(s - sums[:, :SPAN])
        if diagonal:
            weight = jnp.where(seen, weight, 0.0)
        part = dot(weight.astype(BF16), kv[slot, pl.ds(SPAN, SPAN)])
        if diagonal:
            acc[...] = part
            past[...] = sums[:, SPAN:]
        else:
            acc[...] = acc[...] + jnp.exp(-past[...]) * part
            past[...] = past[...] + sums[:, SPAN:]

    def slab_rate(slot):
        rate_now[...] = kv[slot, pl.ds(2 * SPAN, PAD)][:2].astype(F32)

    @pl.when(jnp.logical_not(outset))
    def _():
        q = project(tokens, 0)
        far_sent[...] = q
        split_heads(queries, q)
        slab_rate(0)

    pl.semaphore_wait(bar, expected)

    late_rates = [
        send(rate, late_rate, lr_send.at[i - 1], lr_recv, i, 0) for i in range(1, reach + 1)
    ]
    borrowed = send(tokens, other_tokens, tok_send, tok_recv, 1, 0)

    def w_copy(src, slot, sem, zz, tt):
        return send(src, w_all.at[slot], w_send.at[sem], w_recv.at[slot], zz, tt)

    def across(d):
        return 2 * lax.rem(x + d, chips) + core

    directs = [w_copy(w_out, t, d - 1, z, across(d)) for d in range(1, chips)]
    to_sibling = w_copy(w_out, t, chips - 1, z, sibling)
    passed = [w_copy(w_all.at[across(d)], across(d), chips - 1 + d, z, sibling) for d in range(1, chips)]
    lent = [w_copy(w_out, 0, 2 * chips - 1 + i, 0, p) for i, p in enumerate([1] + list(range(2, ntp, 2)))]
    to_helper = w_copy(w_out, t, 3 * chips - 1, 0, 1)

    def kv_copy(k):
        return send(kv.at[k], kv.at[k + 1], kv_send.at[k], kv_recv.at[k + 1], z + 1, t)

    def mx_copy(p):
        return send(mixed.at[t], mixed.at[t], mx_send.at[p], mx_recv.at[t], z, p)

    def first_copy(p):
        return send(first_mixed, mixed.at[0], mx_send.at[ntp + p], mx_recv.at[0], 0, p)

    ask = send(far_sent, far_in, fq_send, fq_recv, z - far, t)
    answer = send(far_back, far_got, fa_send, fa_recv, z + far, t)

    received = jnp.where(z <= reach, z, far)
    forwarded = jnp.where(last, 0, jnp.where(z + 1 <= reach, z + 1, far))

    @pl.when(outset)
    def _():
        for c in late_rates:
            c.start()

    @pl.when(helper)
    def _():
        borrowed.start()

    @pl.when(jnp.logical_and(jnp.logical_not(outset), forwarded > 0))
    def _():
        kv_copy(0).start()

    @pl.when(guest)
    def _():
        ask.start()

    @pl.when(lead)
    def _():
        for p in range(1, ntp):
            pl.semaphore_signal(late_sem, inc=1, device_id=at(z, p), device_id_type=MESH)

    @pl.when(jnp.logical_not(outset))
    def _():
        for d in range(1, chips):

            @pl.when(across(d) != 0)
            def _():
                directs[d - 1].start()

        @pl.when(sibling != 0)
        def _():
            to_sibling.start()

    @pl.when(deputy)
    def _():
        for c in lent:
            c.start()

    @pl.when(jnp.logical_and(first, jnp.logical_and(core == 0, t != 0)))
    def _():
        to_helper.start()

    def to_lead():
        pl.semaphore_wait(late_sem, 1)
        for d in range(1, chips):

            @pl.when(across(d) == 0)
            def _():
                directs[d - 1].start()

        @pl.when(sibling == 0)
        def _():
            to_sibling.start()

    @pl.when(jnp.logical_and(z > 0, t != 0))
    def _():
        to_lead()

    w_all[t] = w_out[...]

    @pl.when(deputy)
    def _():
        borrowed.wait_recv()
        q = project(other_tokens, 1)
        split_heads(first_queries, q)
        kv_copy(1).start()

    @pl.when(jnp.logical_not(outset))
    def _():
        attend(queries, 0, True)

    def absorb(k, carry):
        @pl.when(jnp.logical_not(deputy))
        def _():
            kv_copy(k - 1).wait_recv()

            @pl.when(k < forwarded)
            def _():
                kv_copy(k).start()

        reaches_first = jnp.logical_and(lead, k == z)

        @pl.when(reaches_first)
        def _():
            late_rates[0].wait_recv()
            rate_now[...] = late_rate[...].astype(F32)

        @pl.when(jnp.logical_not(reaches_first))
        def _():
            slab_rate(k)

        @pl.when(k <= far)
        def _():
            attend(queries, k, False)

        return carry

    lax.fori_loop(1, received + 1, absorb, 0)

    @pl.when(guest)
    def _():
        answer.wait_recv()
        acc[...] = acc[...] + jnp.exp(-past[...]) * jnp.concatenate([far_got[...].astype(F32)] * 2, axis=0)

    @pl.when(jnp.logical_not(outset))
    def _():
        mixed[t] = join_heads(acc[...]).astype(BF16)

    @pl.when(deputy)
    def _():
        rate_now[...] = late_rate[...].astype(F32)
        attend(first_queries, 1, True)
        first_mixed[...] = join_heads(acc[...]).astype(BF16)
        for p in range(ntp):
            first_copy(p).start()

    @pl.when(jnp.logical_not(outset))
    def _():
        for p in range(1, ntp):

            @pl.when(t != p)
            def _():
                mx_copy(p).start()

    @pl.when(jnp.logical_and(z > 0, t != 0))
    def _():
        mx_copy(0).start()

    for d in range(1, chips):

        @pl.when(jnp.logical_not(outset))
        def _():
            w_copy(w_out, across(d), 0, z, t).wait_recv()

        @pl.when(jnp.logical_not(jnp.logical_and(first, x == 0)))
        def _():
            passed[d - 1].start()

    @pl.when(host)
    def _():
        ask.wait_recv()
        split_heads(far_queries, far_in[...])
        acc[...] = jnp.zeros_like(acc)
        past[...] = jnp.zeros_like(past)

        def absorb_far(k, carry):
            reaches_first = jnp.logical_and(lead, k == z)

            @pl.when(reaches_first)
            def _():
                rate_now[...] = late_rate[...].astype(F32)

            @pl.when(jnp.logical_not(reaches_first))
            def _():
                slab_rate(k)

            attend(far_queries, k, False)
            return carry

        lax.fori_loop(1, z + 1, absorb_far, 0)
        far_back[...] = join_heads(acc[...]).astype(BF16)
        answer.start()

    @pl.when(jnp.logical_and(first, t != 0))
    def _():
        to_lead()
        mx_copy(0).start()

    @pl.when(helper)
    def _():
        for d in range(1, chips):
            passed[d - 1].start()

    def wait_w(slot):
        w_copy(w_out, slot, 0, z, t).wait_recv()

    def wait_mixed(slot):
        send(mixed.at[slot], mixed.at[slot], mx_send.at[0], mx_recv.at[slot], z, t).wait_recv()

    for d in range(chips):
        xx = lax.rem(x + d, chips)
        for c in range(2):
            slot = 2 * xx + c
            same = core == c
            own = jnp.logical_and(d == 0, same)
            pl.when(jnp.logical_or(jnp.logical_not(same), jnp.logical_and(outset, d > 0)))(
                functools.partial(wait_w, slot)
            )
            pl.when(jnp.logical_or(jnp.logical_not(own), outset))(functools.partial(wait_mixed, slot))
        pair = jnp.concatenate([mixed[2 * xx], mixed[2 * xx + 1]], axis=1)
        rows = jnp.concatenate([w_all[2 * xx], w_all[2 * xx + 1]], axis=0)
        part = dot(pair, rows)
        if d == 0:
            total[...] = part
        elif d < chips - 1:
            total[...] = total[...] + part
        else:
            out[...] = (total[...] + part).astype(BF16)
    if chips == 1:
        out[...] = total[...].astype(BF16)

    @pl.when(outset)
    def _():
        for c in late_rates:
            c.wait_send()

    @pl.when(helper)
    def _():
        borrowed.wait_send()

    def sent(k, carry):
        kv_copy(k).wait_send()
        return carry

    @pl.when(jnp.logical_not(outset))
    def _():
        lax.fori_loop(0, forwarded, sent, 0)
        for c in directs:
            c.wait_send()
        to_sibling.wait_send()
        for p in range(ntp):

            @pl.when(t != p)
            def _():
                mx_copy(p).wait_send()

    @pl.when(jnp.logical_or(jnp.logical_not(jnp.logical_and(first, x == 0)), helper))
    def _():
        for c in passed:
            c.wait_send()

    @pl.when(deputy)
    def _():
        for c in lent:
            c.wait_send()
        for p in range(ntp):
            first_copy(p).wait_send()

    @pl.when(jnp.logical_and(first, jnp.logical_and(core == 0, t != 0)))
    def _():
        to_helper.wait_send()

    @pl.when(guest)
    def _():
        ask.wait_send()

    @pl.when(host)
    def _():
        answer.wait_send()


def on_device(tokens, norm_gain, w_query, w_key, w_value, w_out, key_rate):
    nsp, ntp = lax.axis_size("sp"), lax.axis_size("tp")
    rows, d = tokens.shape
    width = w_query.shape[1]
    far = nsp // 2 - 1
    chips = ntp // 2
    dma = pltpu.SemaphoreType.DMA
    vmem = pltpu.VMEM
    return pl.pallas_call(
        functools.partial(layer, nsp, ntp, far),
        out_shape=jax.ShapeDtypeStruct((rows, d), BF16),
        in_specs=[pl.BlockSpec(memory_space=pltpu.VMEM)] * 7,
        out_specs=pl.BlockSpec(memory_space=pltpu.VMEM),
        scratch_shapes=[
            vmem((nsp - far + 1, 2 * SPAN + PAD, width), BF16),
            vmem((rows, d), BF16),
            vmem((rows, d), BF16),
            vmem((2 * rows, width), BF16),
            vmem((2 * rows, width), BF16),
            vmem((rows, width), BF16),
            vmem((rows, width), BF16),
            vmem((2 * rows, width), BF16),
            vmem((rows, width), BF16),
            vmem((rows, width), BF16),
            vmem((2 * SPAN, 2 * SPAN), BF16),
            vmem((2, SPAN), F32),
            vmem((2, SPAN), BF16),
            vmem((2 * rows, width), F32),
            vmem((2 * rows, SPAN), F32),
            vmem((ntp, rows, width), BF16),
            vmem((rows, width), BF16),
            vmem((ntp, width, d), BF16),
            vmem((rows, d), F32),
            pltpu.SemaphoreType.REGULAR,
            dma((nsp + 1,)),
            dma((nsp + 1,)),
            dma((3 * chips,)),
            dma((ntp,)),
            dma((2 * ntp,)),
            dma((ntp,)),
            dma,
            dma,
            dma((nsp,)),
            dma,
            dma,
            dma,
            dma,
            dma,
        ],
        compiler_params=pltpu.CompilerParams(
            collective_id=0, has_side_effects=True, vmem_limit_bytes=40 * 1024 * 1024
        ),
    )(tokens, norm_gain.reshape(1, d), w_query, w_key, w_value, w_out, key_rate)


def solution(mesh):
    return jax.shard_map(
        on_device,
        mesh=mesh,
        in_specs=(
            P(("grp", "sp"), None),
            P(),
            P(None, "tp"),
            P(None, "tp"),
            P(None, "tp"),
            P("tp", None),
            P("tp", ("grp", "sp")),
        ),
        out_specs=P(("grp", "sp"), None),
        check_vma=False,
    )
```

```python
import functools

import jax
import jax.numpy as jnp
from jax import lax
from jax.experimental import pallas as pl
from jax.experimental.pallas import tpu as pltpu
from jax.sharding import PartitionSpec as P

HD = 64
SPAN = 128
PAD = 16
VAL = SPAN + PAD
CHUNKS = ((0, VAL), (VAL, SPAN))

F32 = jnp.float32
BF16 = jnp.bfloat16
EPS = 1e-06
MESH = pl.DeviceIdType.MESH


def dot(a, b):
    return lax.dot_general(a, b, (((1,), (0,)), ((), ())), preferred_element_type=F32)


def dot_t(a, b):
    return lax.dot_general(a, b, (((1,), (1,)), ((), ())), preferred_element_type=F32)


def layer(
    nsp,
    ntp,
    far,
    tokens_hbm,
    gain,
    w_query_hbm,
    w_key_hbm,
    w_value_hbm,
    w_out_hbm,
    rate,
    out,
    tokens,
    w_query,
    w_key,
    w_value,
    w_out,
    kv,
    normed,
    other_tokens,
    queries,
    first_q,
    first_queries,
    far_sent,
    far_in,
    far_queries,
    far_back,
    far_got,
    tri,
    rate_now,
    late_rate,
    acc,
    past,
    other_acc,
    other_past,
    mixed,
    first_mixed,
    w_all,
    total,
    late_sem,
    load,
    kv_send,
    kv_recv,
    down_send,
    w_send,
    lent_send,
    w_recv,
    mx_send,
    first_send,
    mx_recv,
    tok_send,
    tok_recv,
    lr_send,
    lr_recv,
    h_send,
    h_recv,
    fq_send,
    fq_recv,
    fa_send,
    fa_recv,
    out_send,
    out_recv,
):
    z = lax.axis_index("sp")
    t = lax.axis_index("tp")
    chips = ntp // 2
    x, core = t // 2, lax.rem(t, 2)
    sibling = 2 * x + 1 - core
    reach = nsp - 1 - far
    lead = t == 0
    first = z == 0
    last = z == nsp - 1
    outset = jnp.logical_and(first, lead)
    deputy = jnp.logical_and(z == 1, lead)
    helper = jnp.logical_and(first, t == 1)
    host = jnp.logical_and(z >= 1, z <= reach)
    guest = z > far

    bar = pltpu.get_barrier_semaphore()

    def at(zz, tt):
        return {"sp": zz, "tp": tt}

    def greet(zz, tt):
        pl.semaphore_signal(bar, inc=1, device_id=at(zz, tt), device_id_type=MESH)

    def send(src, dst, ss, rs, zz, tt):
        return pltpu.make_async_remote_copy(
            src_ref=src, dst_ref=dst, send_sem=ss, recv_sem=rs, device_id=at(zz, tt), device_id_type=MESH
        )

    loads = [
        pltpu.make_async_copy(a, b, load.at[i])
        for i, (a, b) in enumerate(
            (
                (tokens_hbm, tokens),
                (w_key_hbm, w_key),
                (w_value_hbm, w_value),
                (w_query_hbm, w_query),
                (w_out_hbm, w_out),
            )
        )
    ]

    @pl.when(jnp.logical_not(outset))
    def _():
        for c in loads:
            c.start()

    @pl.when(jnp.logical_and(z >= 1, core == 1))
    def _():
        greet(z - 1, t)

    for p in range(ntp):

        @pl.when(jnp.logical_and(t != 0, t != p))
        def _():
            greet(z, p)

    @pl.when(host)
    def _():
        greet(z + far, t)

    @pl.when(jnp.logical_and(host, lead))
    def _():
        greet(0, 0)

    @pl.when(jnp.logical_and(first, t != 0))
    def _():
        greet(1, 0)

    @pl.when(deputy)
    def _():
        greet(0, 1)

    one = lambda flag: jnp.where(flag, 1, 0)
    expected = (
        one(jnp.logical_and(jnp.logical_not(last), core == 1))
        + jnp.where(lead, ntp - 1, ntp - 2)
        + one(guest)
        + one(outset) * reach
        + one(deputy) * (ntp - 1)
        + one(helper)
    )

    @pl.when(jnp.logical_not(outset))
    def _():
        row = lax.broadcasted_iota(jnp.int32, (2 * SPAN, 2 * SPAN), 0)
        col = lax.broadcasted_iota(jnp.int32, (2 * SPAN, 2 * SPAN), 1)
        later = jnp.logical_or(col >= SPAN, lax.rem(row, SPAN) >= col)
        tri[...] = jnp.where(later, 1.0, 0.0).astype(BF16)

    def split_heads(dst, q):
        lane = lax.broadcasted_iota(jnp.int32, (SPAN, 2 * HD), 1)
        qf = q.astype(F32)
        dst[:SPAN] = jnp.where(lane < HD, qf, 0.0).astype(BF16)
        dst[SPAN:] = jnp.where(lane >= HD, qf, 0.0).astype(BF16)

    def join_heads(a):
        lane = lax.broadcasted_iota(jnp.int32, (SPAN, 2 * HD), 1)
        return jnp.where(lane < HD, a[:SPAN], a[SPAN:])

    def project(src, slot, wait):
        wait(0)
        xs = src[...].astype(F32)
        scale = lax.rsqrt(jnp.mean(xs * xs, axis=-1, keepdims=True) + EPS)
        normed[...] = (xs * scale * gain[...]).astype(BF16)
        wait(1)
        kv[slot, core, pl.ds(0, SPAN)] = dot(normed[...], w_key[...]).astype(BF16)
        wait(2)
        kv[slot, core, pl.ds(VAL, SPAN)] = dot(normed[...], w_value[...]).astype(BF16)
        kv[slot, core, pl.ds(SPAN, PAD)] = jnp.concatenate(
            [rate[...].astype(F32), jnp.zeros((PAD - 2, SPAN), F32)], axis=0
        ).astype(BF16)
        wait(3)
        return dot(normed[...], w_query[...]).astype(BF16) * HD ** (-0.5)

    def attend(q_ref, slot, diagonal, acc=acc, past=past, part=core):
        s = dot_t(q_ref[...], kv[slot, part, pl.ds(0, SPAN)])
        s = jnp.concatenate([s[:SPAN] + rate_now[0:1], s[SPAN:] + rate_now[1:2]], axis=0)
        soft = jnp.maximum(s, 0.0) + jnp.log(1.0 + jnp.exp(-jnp.abs(s)))
        if diagonal:
            r = lax.rem(lax.broadcasted_iota(jnp.int32, (2 * SPAN, SPAN), 0), SPAN)
            c = lax.broadcasted_iota(jnp.int32, (2 * SPAN, SPAN), 1)
            seen = c < r
            soft = jnp.where(seen, soft, 0.0)
        high = soft.astype(BF16)
        low = (soft - high.astype(F32)).astype(BF16)
        sums = dot(jnp.concatenate([high, low], axis=1), tri[...])
        weight = jnp.exp(s - sums[:, :SPAN])
        if diagonal:
            weight = jnp.where(seen, weight, 0.0)
        got = dot(weight.astype(BF16), kv[slot, part, pl.ds(VAL, SPAN)])
        if diagonal:
            acc[...] = got
            past[...] = sums[:, SPAN:]
        else:
            acc[...] = acc[...] + jnp.exp(-past[...]) * got
            past[...] = past[...] + sums[:, SPAN:]

    def slab_rate(slot):
        rate_now[...] = kv[slot, core, pl.ds(SPAN, PAD)][:2].astype(F32)

    @pl.when(jnp.logical_not(outset))
    def _():
        q = project(tokens, 0, lambda i: loads[i].wait())
        far_sent[...] = q
        split_heads(queries, q)
        slab_rate(0)
        loads[4].wait()

    pl.semaphore_wait(bar, expected)

    late_rates = [send(rate, late_rate, lr_send.at[0], lr_recv, 0, 1)] + [
        send(rate, late_rate, lr_send.at[1], lr_recv, i, 0) for i in range(1, reach + 1)
    ]
    borrowed = send(tokens, other_tokens, tok_send, tok_recv, 1, 0)

    def w_copy(src, slot, sem, zz, tt):
        return send(src, w_all.at[slot], sem, w_recv.at[slot], zz, tt)

    def across(d):
        return 2 * lax.rem(x + d, chips) + core

    directs = [w_copy(w_out, t, w_send, z, across(d)) for d in range(1, chips)]
    to_sibling = w_copy(w_out, t, w_send, z, sibling)
    passed = [w_copy(w_all.at[across(d)], across(d), w_send, z, sibling) for d in range(1, chips)]
    lent = [w_copy(w_out, 0, lent_send, 0, p) for p in [1] + list(range(2, ntp, 2))]
    to_helper = w_copy(w_out, t, w_send, 0, 1)

    def up(k):
        return [
            send(kv.at[k, :, pl.ds(a, n)], kv.at[k + 1, :, pl.ds(a, n)], kv_send, kv_recv.at[k + 1, c], z + 1, t)
            for c, (a, n) in enumerate(CHUNKS)
        ]

    def down(k):
        return send(kv.at[k, 0], kv.at[k, 0], down_send, kv_recv.at[k, 0], z, sibling)

    def aside(k):
        return send(kv.at[k, 0], kv.at[k, 0], kv_send, kv_recv.at[k, 0], z, sibling)

    alone = send(kv.at[0, 1], kv.at[1, 1], kv_send, kv_recv.at[1, 1], 1, 1)
    back = [
        send(kv.at[1, 0], kv.at[1, 0], h_send.at[0], h_recv.at[0], 0, 1),
        send(first_q, first_q, h_send.at[1], h_recv.at[1], 0, 1),
    ]

    def mx_copy(p):
        return send(mixed.at[t], mixed.at[t], mx_send, mx_recv.at[t], z, p)

    def first_copy(p):
        return send(first_mixed, mixed.at[0], first_send, mx_recv.at[0], 0, p)

    ask = send(far_sent, far_in, fq_send, fq_recv, z - far, t)
    answer = send(far_back, far_got, fa_send, fa_recv, z + far, t)

    first_order = list(range(4, min(6, ntp))) + [p for p in range(2, ntp) if p not in (4, 5)]

    received = jnp.where(z <= reach, z, far)
    forwarded = jnp.where(last, 0, jnp.where(z + 1 <= reach, z + 1, far))

    @pl.when(outset)
    def _():
        for c in late_rates:
            c.start()

    @pl.when(helper)
    def _():
        borrowed.start()

    @pl.when(helper)
    def _():
        alone.start()

    @pl.when(jnp.logical_and(jnp.logical_and(core == 0, jnp.logical_not(outset)), forwarded > 0))
    def _():
        aside(0).start()

    @pl.when(guest)
    def _():
        ask.start()

    for p in range(1, ntp):

        @pl.when(jnp.logical_and(lead, z > 0) if p > 1 else lead)
        def _():
            pl.semaphore_signal(late_sem, inc=1, device_id=at(z, p), device_id_type=MESH)

    @pl.when(jnp.logical_not(outset))
    def _():
        for d in range(1, chips):

            @pl.when(across(d) != 0)
            def _():
                directs[d - 1].start()

        @pl.when(sibling != 0)
        def _():
            to_sibling.start()

    @pl.when(deputy)
    def _():
        for c in lent:
            c.start()

    @pl.when(jnp.logical_and(first, jnp.logical_and(core == 0, t != 0)))
    def _():
        to_helper.start()

    def to_lead():
        pl.semaphore_wait(late_sem, 1)
        for d in range(1, chips):

            @pl.when(across(d) == 0)
            def _():
                directs[d - 1].start()

        @pl.when(sibling == 0)
        def _():
            to_sibling.start()

    @pl.when(jnp.logical_and(z > 0, t != 0))
    def _():
        to_lead()

    @pl.when(jnp.logical_not(outset))
    def _():
        w_all[t] = w_out[...]

    @pl.when(deputy)
    def _():
        borrowed.wait_recv()
        q = project(other_tokens, 1, lambda i: None)
        first_q[...] = q
        aside(1).start()
        for c in back:
            c.start()

    @pl.when(jnp.logical_and(jnp.logical_and(core == 1, forwarded > 0), jnp.logical_not(helper)))
    def _():
        aside(0).wait_recv()
        for c in up(0):
            c.start()

    @pl.when(jnp.logical_not(outset))
    def _():
        attend(queries, 0, True)

    def absorb(k, carry):
        beside = jnp.logical_and(z == 1, t == 1)

        @pl.when(jnp.logical_and(core == 1, jnp.logical_not(beside)))
        def _():
            for c in range(len(CHUNKS)):
                up(k - 1)[c].wait_recv()

                @pl.when(k < forwarded)
                def _():
                    up(k)[c].start()

            down(k).start()

        @pl.when(beside)
        def _():
            alone.wait_recv()
            aside(1).wait_recv()

            @pl.when(k < forwarded)
            def _():
                for c in up(1):
                    c.start()

        @pl.when(jnp.logical_and(core == 0, jnp.logical_not(deputy)))
        def _():
            down(k).wait_recv()

        reaches_first = jnp.logical_and(lead, k == z)

        @pl.when(reaches_first)
        def _():
            late_rates[0].wait_recv()
            rate_now[...] = late_rate[...].astype(F32)

        @pl.when(jnp.logical_not(reaches_first))
        def _():
            slab_rate(k)

        @pl.when(k <= far)
        def _():
            attend(queries, k, False)

        return carry

    lax.fori_loop(1, received + 1, absorb, 0)

    @pl.when(host)
    def _():
        ask.wait_recv()
        split_heads(far_queries, far_in[...])
        other_acc[...] = jnp.zeros_like(other_acc)
        other_past[...] = jnp.zeros_like(other_past)

        def absorb_far(k, carry):
            reaches_first = jnp.logical_and(lead, k == z)

            @pl.when(reaches_first)
            def _():
                rate_now[...] = late_rate[...].astype(F32)

            @pl.when(jnp.logical_not(reaches_first))
            def _():
                slab_rate(k)

            attend(far_queries, k, False, other_acc, other_past)
            return carry

        lax.fori_loop(1, z + 1, absorb_far, 0)
        far_back[...] = join_heads(other_acc[...]).astype(BF16)
        answer.start()

    @pl.when(guest)
    def _():
        answer.wait_recv()
        acc[...] = acc[...] + jnp.exp(-past[...]) * jnp.concatenate([far_got[...].astype(F32)] * 2, axis=0)

    @pl.when(jnp.logical_not(outset))
    def _():
        mixed[t] = join_heads(acc[...]).astype(BF16)

    @pl.when(jnp.logical_not(outset))
    def _():
        for p in range(1, ntp):

            @pl.when(t != p)
            def _():
                mx_copy(p).start()

    @pl.when(jnp.logical_and(z > 0, t != 0))
    def _():
        mx_copy(0).start()

    for d in range(1, chips):

        @pl.when(jnp.logical_not(outset))
        def _():
            w_copy(w_out, across(d), w_send, z, t).wait_recv()

        @pl.when(jnp.logical_not(jnp.logical_and(first, x == 0)))
        def _():
            passed[d - 1].start()

    @pl.when(helper)
    def _():
        for c in back:
            c.wait_recv()
        split_heads(first_queries, first_q[...])
        late_rates[0].wait_recv()
        rate_now[...] = late_rate[...].astype(F32)
        attend(first_queries, 1, True, other_acc, other_past, 0)
        first_mixed[...] = join_heads(other_acc[...]).astype(BF16)
        for p in first_order:
            first_copy(p).start()
        mixed[0] = first_mixed[...]

    def wait_w(slot):
        w_copy(w_out, slot, w_send, z, t).wait_recv()

    def wait_mixed(slot):
        send(mixed.at[slot], mixed.at[slot], mx_send, mx_recv.at[slot], z, t).wait_recv()

    @pl.when(jnp.logical_not(outset))
    def _():
        for xx in list(range(1, chips)) + [0]:
            for slot in (2 * xx, 2 * xx + 1):
                pl.when(core != slot % 2)(functools.partial(wait_w, slot))
                pl.when(jnp.logical_and(t != slot, jnp.logical_not(helper)) if slot == 0 else t != slot)(
                    functools.partial(wait_mixed, slot)
                )
            pair = jnp.concatenate([mixed[2 * xx], mixed[2 * xx + 1]], axis=1)
            rows = jnp.concatenate([w_all[2 * xx], w_all[2 * xx + 1]], axis=0)
            part = dot(pair, rows)
            if xx == 1 or chips == 1:
                total[...] = part
            elif xx > 0:
                total[...] = total[...] + part
            if xx == 0:
                out[...] = (total[...] + part if chips > 1 else part).astype(BF16)

    handed = send(out, out, out_send, out_recv, z, sibling)

    @pl.when(helper)
    def _():
        pl.semaphore_wait(late_sem, 1)
        handed.start()
        handed.wait_send()

    @pl.when(outset)
    def _():
        handed.wait_recv()

    def left(ref, sem):
        send(ref, ref, sem, out_recv, z, sibling).wait_send()

    @pl.when(outset)
    def _():
        left(rate, lr_send.at[0])
        left(kv.at[0, 0, pl.ds(0, 2 * reach)], lr_send.at[1])

    @pl.when(helper)
    def _():
        borrowed.wait_send()
        alone.wait_send()
        if chips > 1:
            left(w_all.at[pl.ds(0, chips - 1)], w_send)
        if ntp > 2:
            left(mixed.at[pl.ds(0, ntp - 2)], first_send)

    carrier = jnp.logical_and(core == 1, jnp.logical_not(helper))
    for n in range(1, reach + 2):

        @pl.when(jnp.logical_and(carrier, forwarded == n))
        def _():
            left(kv.at[pl.ds(0, n)], kv_send)

        if n <= reach:

            @pl.when(jnp.logical_and(jnp.logical_and(core == 1, received == n), jnp.logical_not(jnp.logical_and(z == 1, t == 1))))
            def _():
                left(kv.at[pl.ds(0, n), 0], down_send)

    @pl.when(jnp.logical_and(jnp.logical_and(core == 0, jnp.logical_not(outset)), forwarded > 0))
    def _():
        pl.when(deputy)(lambda: left(kv.at[0], kv_send))
        pl.when(jnp.logical_not(deputy))(lambda: left(kv.at[0, 0], kv_send))

    @pl.when(jnp.logical_not(jnp.logical_and(first, x == 0)))
    def _():
        left(w_all.at[pl.ds(0, ntp - 1)], w_send)

    @pl.when(z > 0)
    def _():
        left(mixed.at[pl.ds(0, ntp - 1)], mx_send)

    if ntp > 2:

        @pl.when(jnp.logical_and(first, t != 0))
        def _():
            left(mixed.at[pl.ds(0, ntp - 2)], mx_send)

    @pl.when(deputy)
    def _():
        left(w_all.at[pl.ds(0, chips)], lent_send)
        for c in back:
            c.wait_send()

    @pl.when(guest)
    def _():
        ask.wait_send()

    @pl.when(host)
    def _():
        answer.wait_send()


def on_device(tokens, norm_gain, w_query, w_key, w_value, w_out, key_rate):
    nsp, ntp = lax.axis_size("sp"), lax.axis_size("tp")
    rows, d = tokens.shape
    width = w_query.shape[1]
    far = nsp // 2 - 1
    chips = ntp // 2
    dma = pltpu.SemaphoreType.DMA
    vmem = pltpu.VMEM
    return pl.pallas_call(
        functools.partial(layer, nsp, ntp, far),
        out_shape=jax.ShapeDtypeStruct((rows, d), BF16),
        in_specs=[pl.BlockSpec(memory_space=pltpu.VMEM if i in (1, 6) else pltpu.HBM) for i in range(7)],
        out_specs=pl.BlockSpec(memory_space=pltpu.VMEM),
        scratch_shapes=[
            vmem((rows, d), BF16),
            vmem((d, width), BF16),
            vmem((d, width), BF16),
            vmem((d, width), BF16),
            vmem((width, d), BF16),
            vmem((nsp - far + 1, 2, 2 * SPAN + PAD, width), BF16),
            vmem((rows, d), BF16),
            vmem((rows, d), BF16),
            vmem((2 * rows, width), BF16),
            vmem((rows, width), BF16),
            vmem((2 * rows, width), BF16),
            vmem((rows, width), BF16),
            vmem((rows, width), BF16),
            vmem((2 * rows, width), BF16),
            vmem((rows, width), BF16),
            vmem((rows, width), BF16),
            vmem((2 * SPAN, 2 * SPAN), BF16),
            vmem((2, SPAN), F32),
            vmem((2, SPAN), BF16),
            vmem((2 * rows, width), F32),
            vmem((2 * rows, SPAN), F32),
            vmem((2 * rows, width), F32),
            vmem((2 * rows, SPAN), F32),
            vmem((ntp, rows, width), BF16),
            vmem((rows, width), BF16),
            vmem((ntp, width, d), BF16),
            vmem((rows, d), F32),
            pltpu.SemaphoreType.REGULAR,
            dma((5,)),
            dma,
            dma((nsp - far + 1, len(CHUNKS))),
            dma,
            dma,
            dma,
            dma((ntp,)),
            dma,
            dma,
            dma((ntp,)),
            dma,
            dma,
            dma((2,)),
            dma,
            dma((2,)),
            dma((2,)),
            dma,
            dma,
            dma,
            dma,
            dma,
            dma,
        ],
        compiler_params=pltpu.CompilerParams(
            collective_id=0, has_side_effects=True, vmem_limit_bytes=60 * 1024 * 1024
        ),
    )(tokens, norm_gain.reshape(1, d), w_query, w_key, w_value, w_out, key_rate)


def solution(mesh):
    return jax.shard_map(
        on_device,
        mesh=mesh,
        in_specs=(
            P(("grp", "sp"), None),
            P(),
            P(None, "tp"),
            P(None, "tp"),
            P(None, "tp"),
            P("tp", None),
            P("tp", ("grp", "sp")),
        ),
        out_specs=P(("grp", "sp"), None),
        check_vma=False,
    )
```

```python
import functools

import jax
import jax.numpy as jnp
from jax import lax
from jax.experimental import pallas as pl
from jax.experimental.pallas import tpu as pltpu
from jax.sharding import PartitionSpec as P

HD = 64
SPAN = 128
PAD = 16
VAL = SPAN + PAD
CHUNKS = ((0, VAL), (VAL, SPAN))

F32 = jnp.float32
BF16 = jnp.bfloat16
EPS = 1e-06
MESH = pl.DeviceIdType.MESH


def dot(a, b):
    return lax.dot_general(a, b, (((1,), (0,)), ((), ())), preferred_element_type=F32)


def dot_t(a, b):
    return lax.dot_general(a, b, (((1,), (1,)), ((), ())), preferred_element_type=F32)


def layer(
    nsp,
    ntp,
    far,
    tokens_hbm,
    gain,
    w_query_hbm,
    w_key_hbm,
    w_value_hbm,
    w_out_hbm,
    rate,
    out,
    tokens,
    w_query,
    w_key,
    w_value,
    w_out,
    kv,
    normed,
    other_tokens,
    queries,
    first_q,
    first_queries,
    far_sent,
    far_in,
    far_queries,
    far_back,
    far_got,
    tri,
    rate_now,
    late_rate,
    late_span,
    acc,
    past,
    other_acc,
    other_past,
    mixed,
    first_mixed,
    w_all,
    total,
    late_sem,
    load,
    kv_send,
    kv_recv,
    down_send,
    w_send,
    lent_send,
    w_recv,
    mx_send,
    first_send,
    mx_recv,
    tok_send,
    tok_recv,
    lr_send,
    lr_recv,
    h_send,
    h_recv,
    fq_send,
    fq_recv,
    fa_send,
    fa_recv,
    out_send,
    out_recv,
):
    z = lax.axis_index("sp")
    t = lax.axis_index("tp")
    chips = ntp // 2
    x, core = t // 2, lax.rem(t, 2)
    sibling = 2 * x + 1 - core
    reach = nsp - 1 - far
    most = max(far, reach)
    lead = t == 0
    first = z == 0
    last = z == nsp - 1
    outset = jnp.logical_and(first, lead)
    deputy = jnp.logical_and(z == 1, lead)
    helper = jnp.logical_and(first, t == 1)
    host = jnp.logical_and(z >= 1, z <= reach)
    guest = z > far

    bar = pltpu.get_barrier_semaphore()

    def at(zz, tt):
        return {"sp": zz, "tp": tt}

    def greet(zz, tt):
        pl.semaphore_signal(bar, inc=1, device_id=at(zz, tt), device_id_type=MESH)

    def send(src, dst, ss, rs, zz, tt):
        return pltpu.make_async_remote_copy(
            src_ref=src, dst_ref=dst, send_sem=ss, recv_sem=rs, device_id=at(zz, tt), device_id_type=MESH
        )

    loads = [
        pltpu.make_async_copy(a, b, load.at[i])
        for i, (a, b) in enumerate(
            (
                (tokens_hbm, tokens),
                (w_key_hbm, w_key),
                (w_value_hbm, w_value),
                (w_query_hbm, w_query),
                (w_out_hbm, w_out),
            )
        )
    ]

    @pl.when(jnp.logical_not(outset))
    def _():
        for c in loads:
            c.start()

    @pl.when(jnp.logical_and(z >= 1, core == 1))
    def _():
        greet(z - 1, t)

    for p in range(ntp):

        @pl.when(jnp.logical_and(t != 0, t != p))
        def _():
            greet(z, p)

    @pl.when(host)
    def _():
        greet(z + far, t)

    @pl.when(jnp.logical_and(jnp.logical_and(z >= 1, z <= most), lead))
    def _():
        greet(0, 0)

    @pl.when(jnp.logical_and(first, t != 0))
    def _():
        greet(1, 0)

    @pl.when(deputy)
    def _():
        greet(0, 1)

    one = lambda flag: jnp.where(flag, 1, 0)
    expected = (
        one(jnp.logical_and(jnp.logical_not(last), core == 1))
        + jnp.where(lead, ntp - 1, ntp - 2)
        + one(guest)
        + one(outset) * most
        + one(deputy) * (ntp - 1)
        + one(helper)
    )

    @pl.when(jnp.logical_not(outset))
    def _():
        row = lax.broadcasted_iota(jnp.int32, (2 * SPAN, 2 * SPAN), 0)
        col = lax.broadcasted_iota(jnp.int32, (2 * SPAN, 2 * SPAN), 1)
        later = jnp.logical_or(col >= SPAN, lax.rem(row, SPAN) >= col)
        tri[...] = jnp.where(later, 1.0, 0.0).astype(BF16)

    def split_heads(dst, q):
        lane = lax.broadcasted_iota(jnp.int32, (SPAN, 2 * HD), 1)
        qf = q.astype(F32)
        dst[:SPAN] = jnp.where(lane < HD, qf, 0.0).astype(BF16)
        dst[SPAN:] = jnp.where(lane >= HD, qf, 0.0).astype(BF16)

    def join_heads(a):
        lane = lax.broadcasted_iota(jnp.int32, (SPAN, 2 * HD), 1)
        return jnp.where(lane < HD, a[:SPAN], a[SPAN:])

    def project(src, slot, wait):
        wait(0)
        xs = src[...].astype(F32)
        scale = lax.rsqrt(jnp.mean(xs * xs, axis=-1, keepdims=True) + EPS)
        normed[...] = (xs * scale * gain[...]).astype(BF16)
        wait(1)
        kv[slot, core, pl.ds(0, SPAN)] = dot(normed[...], w_key[...]).astype(BF16)
        wait(2)
        kv[slot, core, pl.ds(VAL, SPAN)] = dot(normed[...], w_value[...]).astype(BF16)
        kv[slot, core, pl.ds(SPAN, PAD)] = jnp.concatenate(
            [rate[...].astype(F32), jnp.zeros((PAD - 2, SPAN), F32)], axis=0
        ).astype(BF16)
        wait(3)
        return dot(normed[...], w_query[...]).astype(BF16) * HD ** (-0.5)

    def attend(q_ref, slot, diagonal, acc=acc, past=past, part=core):
        s = dot_t(q_ref[...], kv[slot, part, pl.ds(0, SPAN)])
        s = jnp.concatenate([s[:SPAN] + rate_now[0:1], s[SPAN:] + rate_now[1:2]], axis=0)
        soft = jnp.maximum(s, 0.0) + jnp.log(1.0 + jnp.exp(-jnp.abs(s)))
        if diagonal:
            r = lax.rem(lax.broadcasted_iota(jnp.int32, (2 * SPAN, SPAN), 0), SPAN)
            c = lax.broadcasted_iota(jnp.int32, (2 * SPAN, SPAN), 1)
            seen = c < r
            soft = jnp.where(seen, soft, 0.0)
        high = soft.astype(BF16)
        low = (soft - high.astype(F32)).astype(BF16)
        sums = dot(jnp.concatenate([high, low], axis=1), tri[...])
        weight = jnp.exp(s - sums[:, :SPAN])
        if diagonal:
            weight = jnp.where(seen, weight, 0.0)
        got = dot(weight.astype(BF16), kv[slot, part, pl.ds(VAL, SPAN)])
        if diagonal:
            acc[...] = got
            past[...] = sums[:, SPAN:]
        else:
            acc[...] = acc[...] + jnp.exp(-past[...]) * got
            past[...] = past[...] + sums[:, SPAN:]

    def slab_rate(slot):
        rate_now[...] = kv[slot, core, pl.ds(SPAN, PAD)][:2].astype(F32)

    @pl.when(jnp.logical_not(outset))
    def _():
        q = project(tokens, 0, lambda i: loads[i].wait())
        far_sent[...] = q
        split_heads(queries, q)
        slab_rate(0)
        loads[4].wait()

    pl.semaphore_wait(bar, expected)

    late_rates = [send(rate, late_rate, lr_send.at[0], lr_recv, 0, 1)] + [
        send(rate, late_rate, lr_send.at[1], lr_recv, i, 0) for i in range(1, most + 1)
    ]
    borrowed = send(tokens, other_tokens, tok_send, tok_recv, 1, 0)

    def w_copy(src, slot, sem, zz, tt):
        return send(src, w_all.at[slot], sem, w_recv.at[slot], zz, tt)

    def across(d):
        return 2 * lax.rem(x + d, chips) + core

    directs = [w_copy(w_out, t, w_send, z, across(d)) for d in range(1, chips)]
    to_sibling = w_copy(w_out, t, w_send, z, sibling)
    passed = [w_copy(w_all.at[across(d)], across(d), w_send, z, sibling) for d in range(1, chips)]
    lent = [w_copy(w_out, 0, lent_send, 0, p) for p in [1] + list(range(2, ntp, 2))]
    to_helper = w_copy(w_out, t, w_send, 0, 1)

    def up(k):
        return [
            send(kv.at[k, :, pl.ds(a, n)], kv.at[k + 1, :, pl.ds(a, n)], kv_send, kv_recv.at[k + 1, c], z + 1, t)
            for c, (a, n) in enumerate(CHUNKS)
        ]

    def down(k):
        return send(kv.at[k, 0], kv.at[k, 0], down_send, kv_recv.at[k, 0], z, sibling)

    def aside(k):
        return send(kv.at[k, 0], kv.at[k, 0], kv_send, kv_recv.at[k, 0], z, sibling)

    alone = send(kv.at[0, 1], kv.at[1, 1], kv_send, kv_recv.at[1, 1], 1, 1)
    back = [
        send(kv.at[1, 0], kv.at[1, 0], h_send.at[0], h_recv.at[0], 0, 1),
        send(first_q, first_q, h_send.at[1], h_recv.at[1], 0, 1),
    ]

    def mx_copy(p):
        return send(mixed.at[t], mixed.at[t], mx_send, mx_recv.at[t], z, p)

    def first_copy(p):
        return send(first_mixed, mixed.at[0], first_send, mx_recv.at[0], 0, p)

    ask = send(far_sent, far_in, fq_send, fq_recv, z - far, t)
    answer = send(far_back, far_got, fa_send, fa_recv, z + far, t)

    first_order = list(range(4, min(6, ntp))) + [p for p in range(2, ntp) if p not in (4, 5)]

    def needed(zz):
        return jnp.where(zz <= reach, zz, jnp.minimum(zz, far))

    received = needed(z)
    forwarded = jnp.where(last, 0, needed(z + 1))

    @pl.when(outset)
    def _():
        for c in late_rates:
            c.start()

    @pl.when(helper)
    def _():
        borrowed.start()

    @pl.when(helper)
    def _():
        alone.start()

    @pl.when(jnp.logical_and(jnp.logical_and(core == 0, jnp.logical_not(outset)), forwarded > 0))
    def _():
        aside(0).start()

    @pl.when(guest)
    def _():
        ask.start()

    for p in range(1, ntp):

        @pl.when(jnp.logical_and(lead, z > 0) if p > 1 else lead)
        def _():
            pl.semaphore_signal(late_sem, inc=1, device_id=at(z, p), device_id_type=MESH)

    @pl.when(jnp.logical_not(outset))
    def _():
        for d in range(1, chips):

            @pl.when(across(d) != 0)
            def _():
                directs[d - 1].start()

        @pl.when(sibling != 0)
        def _():
            to_sibling.start()

    @pl.when(deputy)
    def _():
        for c in lent:
            c.start()

    @pl.when(jnp.logical_and(first, jnp.logical_and(core == 0, t != 0)))
    def _():
        to_helper.start()

    def to_lead():
        pl.semaphore_wait(late_sem, 1)
        for d in range(1, chips):

            @pl.when(across(d) == 0)
            def _():
                directs[d - 1].start()

        @pl.when(sibling == 0)
        def _():
            to_sibling.start()

    @pl.when(jnp.logical_and(z > 0, t != 0))
    def _():
        to_lead()

    @pl.when(jnp.logical_not(outset))
    def _():
        w_all[t] = w_out[...]

    @pl.when(deputy)
    def _():
        borrowed.wait_recv()
        q = project(other_tokens, 1, lambda i: None)
        first_q[...] = q
        aside(1).start()
        for c in back:
            c.start()

    @pl.when(jnp.logical_and(jnp.logical_and(core == 1, forwarded > 0), jnp.logical_not(helper)))
    def _():
        aside(0).wait_recv()
        for c in up(0):
            c.start()

    @pl.when(jnp.logical_not(outset))
    def _():
        attend(queries, 0, True)

    def absorb(k, carry):
        beside = jnp.logical_and(z == 1, t == 1)

        @pl.when(jnp.logical_and(core == 1, jnp.logical_not(beside)))
        def _():
            for c in range(len(CHUNKS)):
                up(k - 1)[c].wait_recv()

                @pl.when(k < forwarded)
                def _():
                    up(k)[c].start()

            down(k).start()

        @pl.when(beside)
        def _():
            alone.wait_recv()
            aside(1).wait_recv()

            @pl.when(k < forwarded)
            def _():
                for c in up(1):
                    c.start()

        @pl.when(jnp.logical_and(core == 0, jnp.logical_not(deputy)))
        def _():
            down(k).wait_recv()

        reaches_first = jnp.logical_and(lead, k == z)

        @pl.when(reaches_first)
        def _():
            late_rates[0].wait_recv()
            rate_now[...] = late_rate[...].astype(F32)

        @pl.when(jnp.logical_not(reaches_first))
        def _():
            slab_rate(k)

        @pl.when(k <= far)
        def _():
            attend(queries, k, False)

        return carry

    lax.fori_loop(1, received + 1, absorb, 0)

    @pl.when(guest)
    def _():
        answer.wait_recv()
        acc[...] = acc[...] + jnp.exp(-past[...]) * jnp.concatenate([far_got[...].astype(F32)] * 2, axis=0)

    @pl.when(jnp.logical_not(outset))
    def _():
        mixed[t] = join_heads(acc[...]).astype(BF16)

    @pl.when(jnp.logical_not(outset))
    def _():
        for p in range(1, ntp):

            @pl.when(t != p)
            def _():
                mx_copy(p).start()

    @pl.when(jnp.logical_and(z > 0, t != 0))
    def _():
        mx_copy(0).start()

    for d in range(1, chips):

        @pl.when(jnp.logical_not(outset))
        def _():
            w_copy(w_out, across(d), w_send, z, t).wait_recv()

        @pl.when(jnp.logical_not(jnp.logical_and(first, x == 0)))
        def _():
            passed[d - 1].start()

    @pl.when(host)
    def _():
        ask.wait_recv()
        split_heads(far_queries, far_in[...])
        other_acc[...] = jnp.zeros_like(other_acc)
        other_past[...] = jnp.zeros_like(other_past)

        def absorb_far(k, carry):
            reaches_first = jnp.logical_and(lead, k == z)

            @pl.when(reaches_first)
            def _():
                rate_now[...] = late_rate[...].astype(F32)

            @pl.when(jnp.logical_not(reaches_first))
            def _():
                slab_rate(k)

            attend(far_queries, k, False, other_acc, other_past)
            return carry

        lax.fori_loop(1, z + 1, absorb_far, 0)
        far_back[...] = join_heads(other_acc[...]).astype(BF16)
        answer.start()

    def wait_w(slot):
        w_copy(w_out, slot, w_send, z, t).wait_recv()

    def wait_mixed(slot):
        send(mixed.at[slot], mixed.at[slot], mx_send, mx_recv.at[slot], z, t).wait_recv()

    def project_out(xx):
        for slot in (2 * xx, 2 * xx + 1):
            pl.when(core != slot % 2)(functools.partial(wait_w, slot))
            pl.when(jnp.logical_and(t != slot, jnp.logical_not(helper)) if slot == 0 else t != slot)(
                functools.partial(wait_mixed, slot)
            )
        pair = jnp.concatenate([mixed[2 * xx], mixed[2 * xx + 1]], axis=1)
        rows = jnp.concatenate([w_all[2 * xx], w_all[2 * xx + 1]], axis=0)
        got = dot(pair, rows)
        if xx == 1 and chips > 1:
            total[...] = got
        elif xx > 0:
            total[...] = total[...] + got
        else:
            out[...] = (total[...] + got if chips > 1 else got).astype(BF16)

    @pl.when(jnp.logical_not(outset))
    def _():
        for xx in range(1, chips):
            project_out(xx)

    @pl.when(helper)
    def _():
        for c in back:
            c.wait_recv()
        split_heads(first_queries, first_q[...])
        late_rates[0].wait_recv()
        rate_now[...] = late_rate[...].astype(F32)
        attend(first_queries, 1, True, other_acc, other_past, 0)
        first_mixed[...] = join_heads(other_acc[...]).astype(BF16)
        for p in first_order:
            first_copy(p).start()
        mixed[0] = first_mixed[...]

    @pl.when(jnp.logical_not(outset))
    def _():
        project_out(0)

    handed = send(out, out, out_send, out_recv, z, sibling)

    @pl.when(helper)
    def _():
        pl.semaphore_wait(late_sem, 1)
        handed.start()
        handed.wait_send()

    @pl.when(outset)
    def _():
        handed.wait_recv()

    def left(ref, sem):
        send(ref, ref, sem, out_recv, z, sibling).wait_send()

    @pl.when(outset)
    def _():
        left(rate, lr_send.at[0])
        left(late_span, lr_send.at[1])

    @pl.when(helper)
    def _():
        borrowed.wait_send()
        alone.wait_send()
        if chips > 1:
            left(w_all.at[pl.ds(0, chips - 1)], w_send)
        if ntp > 2:
            left(mixed.at[pl.ds(0, ntp - 2)], first_send)

    carrier = jnp.logical_and(core == 1, jnp.logical_not(helper))
    for n in range(1, most + 1):

        @pl.when(jnp.logical_and(carrier, forwarded == n))
        def _():
            left(kv.at[pl.ds(0, n)], kv_send)

        @pl.when(
            jnp.logical_and(
                jnp.logical_and(core == 1, received == n), jnp.logical_not(jnp.logical_and(z == 1, t == 1))
            )
        )
        def _():
            left(kv.at[pl.ds(0, n), 0], down_send)

    @pl.when(jnp.logical_and(jnp.logical_and(core == 0, jnp.logical_not(outset)), forwarded > 0))
    def _():
        pl.when(deputy)(lambda: left(kv.at[0], kv_send))
        pl.when(jnp.logical_not(deputy))(lambda: left(kv.at[0, 0], kv_send))

    @pl.when(jnp.logical_not(jnp.logical_and(first, x == 0)))
    def _():
        left(w_all.at[pl.ds(0, ntp - 1)], w_send)

    @pl.when(z > 0)
    def _():
        left(mixed.at[pl.ds(0, ntp - 1)], mx_send)

    if ntp > 2:

        @pl.when(jnp.logical_and(first, t != 0))
        def _():
            left(mixed.at[pl.ds(0, ntp - 2)], mx_send)

    @pl.when(deputy)
    def _():
        left(w_all.at[pl.ds(0, chips)], lent_send)
        for c in back:
            c.wait_send()

    @pl.when(guest)
    def _():
        ask.wait_send()

    @pl.when(host)
    def _():
        answer.wait_send()


def on_device(tokens, norm_gain, w_query, w_key, w_value, w_out, key_rate):
    nsp, ntp = lax.axis_size("sp"), lax.axis_size("tp")
    rows, d = tokens.shape
    width = w_query.shape[1]
    far = nsp // 2
    most = max(far, nsp - 1 - far)
    chips = ntp // 2
    dma = pltpu.SemaphoreType.DMA
    vmem = pltpu.VMEM
    return pl.pallas_call(
        functools.partial(layer, nsp, ntp, far),
        out_shape=jax.ShapeDtypeStruct((rows, d), BF16),
        in_specs=[pl.BlockSpec(memory_space=pltpu.VMEM if i in (1, 6) else pltpu.HBM) for i in range(7)],
        out_specs=pl.BlockSpec(memory_space=pltpu.VMEM),
        scratch_shapes=[
            vmem((rows, d), BF16),
            vmem((d, width), BF16),
            vmem((d, width), BF16),
            vmem((d, width), BF16),
            vmem((width, d), BF16),
            vmem((most + 1, 2, 2 * SPAN + PAD, width), BF16),
            vmem((rows, d), BF16),
            vmem((rows, d), BF16),
            vmem((2 * rows, width), BF16),
            vmem((rows, width), BF16),
            vmem((2 * rows, width), BF16),
            vmem((rows, width), BF16),
            vmem((rows, width), BF16),
            vmem((2 * rows, width), BF16),
            vmem((rows, width), BF16),
            vmem((rows, width), BF16),
            vmem((2 * SPAN, 2 * SPAN), BF16),
            vmem((2, SPAN), F32),
            vmem((2, SPAN), BF16),
            vmem((most, 2, SPAN), BF16),
            vmem((2 * rows, width), F32),
            vmem((2 * rows, SPAN), F32),
            vmem((2 * rows, width), F32),
            vmem((2 * rows, SPAN), F32),
            vmem((ntp, rows, width), BF16),
            vmem((rows, width), BF16),
            vmem((ntp, width, d), BF16),
            vmem((rows, d), F32),
            pltpu.SemaphoreType.REGULAR,
            dma((5,)),
            dma,
            dma((most + 1, len(CHUNKS))),
            dma,
            dma,
            dma,
            dma((ntp,)),
            dma,
            dma,
            dma((ntp,)),
            dma,
            dma,
            dma((2,)),
            dma,
            dma((2,)),
            dma((2,)),
            dma,
            dma,
            dma,
            dma,
            dma,
            dma,
        ],
        compiler_params=pltpu.CompilerParams(
            collective_id=0, has_side_effects=True, vmem_limit_bytes=60 * 1024 * 1024
        ),
    )(tokens, norm_gain.reshape(1, d), w_query, w_key, w_value, w_out, key_rate)


def solution(mesh):
    return jax.shard_map(
        on_device,
        mesh=mesh,
        in_specs=(
            P(("grp", "sp"), None),
            P(),
            P(None, "tp"),
            P(None, "tp"),
            P(None, "tp"),
            P("tp", None),
            P("tp", ("grp", "sp")),
        ),
        out_specs=P(("grp", "sp"), None),
        check_vma=False,
    )
```

```python
import functools

import jax
import jax.numpy as jnp
from jax import lax
from jax.experimental import pallas as pl
from jax.experimental.pallas import tpu as pltpu
from jax.sharding import PartitionSpec as P

HD = 64
SPAN = 128
PAD = 16
VAL = SPAN + PAD
CHUNKS = ((0, VAL), (VAL, SPAN))

F32 = jnp.float32
BF16 = jnp.bfloat16
EPS = 1e-06
MESH = pl.DeviceIdType.MESH


def dot(a, b):
    return lax.dot_general(a, b, (((1,), (0,)), ((), ())), preferred_element_type=F32)


def dot_t(a, b):
    return lax.dot_general(a, b, (((1,), (1,)), ((), ())), preferred_element_type=F32)


def layer(
    nsp,
    ntp,
    far,
    tokens_hbm,
    gain,
    w_query_hbm,
    w_key_hbm,
    w_value_hbm,
    w_out_hbm,
    rate,
    out,
    tokens,
    w_query,
    w_key,
    w_value,
    w_out,
    kv,
    normed,
    other_tokens,
    queries,
    first_q,
    first_queries,
    far_sent,
    far_in,
    far_queries,
    far_back,
    far_got,
    tri,
    rate_now,
    late_rate,
    late_span,
    acc,
    past,
    other_acc,
    other_past,
    mixed,
    first_mixed,
    w_all,
    total,
    late_sem,
    load,
    kv_send,
    kv_recv,
    down_send,
    w_send,
    lent_send,
    w_recv,
    mx_send,
    first_send,
    mx_recv,
    tok_send,
    tok_recv,
    lr_send,
    lr_recv,
    h_send,
    h_recv,
    fq_send,
    fq_recv,
    fa_send,
    fa_recv,
    out_send,
    out_recv,
):
    z = lax.axis_index("sp")
    t = lax.axis_index("tp")
    chips = ntp // 2
    x, core = t // 2, lax.rem(t, 2)
    sibling = 2 * x + 1 - core
    reach = nsp - 1 - far
    most = max(far, reach)
    lead = t == 0
    first = z == 0
    last = z == nsp - 1
    outset = jnp.logical_and(first, lead)
    deputy = jnp.logical_and(z == 1, lead)
    helper = jnp.logical_and(first, t == 1)
    host = jnp.logical_and(z >= 1, z <= reach)
    guest = z > far

    bar = pltpu.get_barrier_semaphore()

    def at(zz, tt):
        return {"sp": zz, "tp": tt}

    def greet(zz, tt):
        pl.semaphore_signal(bar, inc=1, device_id=at(zz, tt), device_id_type=MESH)

    def send(src, dst, ss, rs, zz, tt):
        return pltpu.make_async_remote_copy(
            src_ref=src, dst_ref=dst, send_sem=ss, recv_sem=rs, device_id=at(zz, tt), device_id_type=MESH
        )

    loads = [
        pltpu.make_async_copy(a, b, load.at[i])
        for i, (a, b) in enumerate(
            (
                (tokens_hbm, tokens),
                (w_key_hbm, w_key),
                (w_value_hbm, w_value),
                (w_query_hbm, w_query),
                (w_out_hbm, w_out),
            )
        )
    ]

    @pl.when(jnp.logical_not(outset))
    def _():
        for c in loads:
            c.start()

    @pl.when(jnp.logical_and(z >= 1, core == 1))
    def _():
        greet(z - 1, t)

    for p in range(ntp):

        @pl.when(jnp.logical_and(t != 0, t != p))
        def _():
            greet(z, p)

    @pl.when(host)
    def _():
        greet(z + far, t)

    @pl.when(jnp.logical_and(jnp.logical_and(z >= 1, z <= most), lead))
    def _():
        greet(0, 0)

    @pl.when(jnp.logical_and(first, t != 0))
    def _():
        greet(1, 0)

    @pl.when(deputy)
    def _():
        greet(0, 1)

    one = lambda flag: jnp.where(flag, 1, 0)
    expected = (
        one(jnp.logical_and(jnp.logical_not(last), core == 1))
        + jnp.where(lead, ntp - 1, ntp - 2)
        + one(guest)
        + one(outset) * most
        + one(deputy) * (ntp - 1)
        + one(helper)
    )

    late_rates = [send(rate, late_rate, lr_send.at[0], lr_recv, 0, 1)] + [
        send(rate, late_rate, lr_send.at[1], lr_recv, i, 0) for i in range(1, most + 1)
    ]

    @pl.when(outset)
    def _():
        pl.semaphore_wait(bar, expected)
        for c in late_rates:
            c.start()

    @pl.when(jnp.logical_not(outset))
    def _():
        row = lax.broadcasted_iota(jnp.int32, (2 * SPAN, 2 * SPAN), 0)
        col = lax.broadcasted_iota(jnp.int32, (2 * SPAN, 2 * SPAN), 1)
        later = jnp.logical_or(col >= SPAN, lax.rem(row, SPAN) >= col)
        tri[...] = jnp.where(later, 1.0, 0.0).astype(BF16)

    def split_heads(dst, q):
        lane = lax.broadcasted_iota(jnp.int32, (SPAN, 2 * HD), 1)
        qf = q.astype(F32)
        dst[:SPAN] = jnp.where(lane < HD, qf, 0.0).astype(BF16)
        dst[SPAN:] = jnp.where(lane >= HD, qf, 0.0).astype(BF16)

    def join_heads(a):
        lane = lax.broadcasted_iota(jnp.int32, (SPAN, 2 * HD), 1)
        return jnp.where(lane < HD, a[:SPAN], a[SPAN:])

    def project(src, slot, wait):
        wait(0)
        xs = src[...].astype(F32)
        scale = lax.rsqrt(jnp.mean(xs * xs, axis=-1, keepdims=True) + EPS)
        normed[...] = (xs * scale * gain[...]).astype(BF16)
        wait(1)
        kv[slot, core, pl.ds(0, SPAN)] = dot(normed[...], w_key[...]).astype(BF16)
        wait(2)
        kv[slot, core, pl.ds(VAL, SPAN)] = dot(normed[...], w_value[...]).astype(BF16)
        kv[slot, core, pl.ds(SPAN, PAD)] = jnp.concatenate(
            [rate[...].astype(F32), jnp.zeros((PAD - 2, SPAN), F32)], axis=0
        ).astype(BF16)
        wait(3)
        return dot(normed[...], w_query[...]).astype(BF16) * HD ** (-0.5)

    def attend(q_ref, slot, diagonal, acc=acc, past=past, part=core):
        s = dot_t(q_ref[...], kv[slot, part, pl.ds(0, SPAN)])
        s = jnp.concatenate([s[:SPAN] + rate_now[0:1], s[SPAN:] + rate_now[1:2]], axis=0)
        soft = jnp.maximum(s, 0.0) + jnp.log(1.0 + jnp.exp(-jnp.abs(s)))
        if diagonal:
            r = lax.rem(lax.broadcasted_iota(jnp.int32, (2 * SPAN, SPAN), 0), SPAN)
            c = lax.broadcasted_iota(jnp.int32, (2 * SPAN, SPAN), 1)
            seen = c < r
            soft = jnp.where(seen, soft, 0.0)
        high = soft.astype(BF16)
        low = (soft - high.astype(F32)).astype(BF16)
        sums = dot(jnp.concatenate([high, low], axis=1), tri[...])
        weight = jnp.exp(s - sums[:, :SPAN])
        if diagonal:
            weight = jnp.where(seen, weight, 0.0)
        got = dot(weight.astype(BF16), kv[slot, part, pl.ds(VAL, SPAN)])
        if diagonal:
            acc[...] = got
            past[...] = sums[:, SPAN:]
        else:
            acc[...] = acc[...] + jnp.exp(-past[...]) * got
            past[...] = past[...] + sums[:, SPAN:]

    def slab_rate(slot):
        rate_now[...] = kv[slot, core, pl.ds(SPAN, PAD)][:2].astype(F32)

    @pl.when(jnp.logical_not(outset))
    def _():
        q = project(tokens, 0, lambda i: loads[i].wait())
        far_sent[...] = q
        split_heads(queries, q)
        slab_rate(0)
        loads[4].wait()

    @pl.when(jnp.logical_not(outset))
    def _():
        pl.semaphore_wait(bar, expected)

    borrowed = send(tokens, other_tokens, tok_send, tok_recv, 1, 0)

    def w_copy(src, slot, sem, zz, tt):
        return send(src, w_all.at[slot], sem, w_recv.at[slot], zz, tt)

    def across(d):
        return 2 * lax.rem(x + d, chips) + core

    directs = [w_copy(w_out, t, w_send, z, across(d)) for d in range(1, chips)]
    to_sibling = w_copy(w_out, t, w_send, z, sibling)
    passed = [w_copy(w_all.at[across(d)], across(d), w_send, z, sibling) for d in range(1, chips)]
    lent = [w_copy(w_out, 0, lent_send, 0, p) for p in [1] + list(range(2, ntp, 2))]
    to_helper = w_copy(w_out, t, w_send, 0, 1)

    def up(k):
        return [
            send(kv.at[k, :, pl.ds(a, n)], kv.at[k + 1, :, pl.ds(a, n)], kv_send, kv_recv.at[k + 1, c], z + 1, t)
            for c, (a, n) in enumerate(CHUNKS)
        ]

    def down(k):
        return send(kv.at[k, 0], kv.at[k, 0], down_send, kv_recv.at[k, 0], z, sibling)

    def aside(k):
        return send(kv.at[k, 0], kv.at[k, 0], kv_send, kv_recv.at[k, 0], z, sibling)

    alone = send(kv.at[0, 1], kv.at[1, 1], kv_send, kv_recv.at[1, 1], 1, 1)
    back = [
        send(kv.at[1, 0], kv.at[1, 0], h_send.at[0], h_recv.at[0], 0, 1),
        send(first_q, first_q, h_send.at[1], h_recv.at[1], 0, 1),
    ]

    def mx_copy(p):
        return send(mixed.at[t], mixed.at[t], mx_send, mx_recv.at[t], z, p)

    def first_copy(p):
        return send(first_mixed, mixed.at[0], first_send, mx_recv.at[0], 0, p)

    ask = send(far_sent, far_in, fq_send, fq_recv, z - far, t)
    answer = send(far_back, far_got, fa_send, fa_recv, z + far, t)

    first_order = list(range(4, min(6, ntp))) + [p for p in range(2, ntp) if p not in (4, 5)]

    def needed(zz):
        return jnp.where(zz <= reach, zz, jnp.minimum(zz, far))

    received = needed(z)
    forwarded = jnp.where(last, 0, needed(z + 1))

    @pl.when(helper)
    def _():
        borrowed.start()

    @pl.when(helper)
    def _():
        alone.start()

    @pl.when(jnp.logical_and(jnp.logical_and(core == 0, jnp.logical_not(outset)), forwarded > 0))
    def _():
        aside(0).start()

    @pl.when(guest)
    def _():
        ask.start()

    for p in range(1, ntp):

        @pl.when(jnp.logical_and(lead, z > 0) if p > 1 else lead)
        def _():
            pl.semaphore_signal(late_sem, inc=1, device_id=at(z, p), device_id_type=MESH)

    @pl.when(jnp.logical_not(outset))
    def _():
        for d in range(1, chips):

            @pl.when(across(d) != 0)
            def _():
                directs[d - 1].start()

        @pl.when(sibling != 0)
        def _():
            to_sibling.start()

    @pl.when(deputy)
    def _():
        for c in lent:
            c.start()

    @pl.when(jnp.logical_and(first, jnp.logical_and(core == 0, t != 0)))
    def _():
        to_helper.start()

    def to_lead():
        pl.semaphore_wait(late_sem, 1)
        for d in range(1, chips):

            @pl.when(across(d) == 0)
            def _():
                directs[d - 1].start()

        @pl.when(sibling == 0)
        def _():
            to_sibling.start()

    @pl.when(jnp.logical_and(z > 0, t != 0))
    def _():
        to_lead()

    @pl.when(jnp.logical_not(outset))
    def _():
        w_all[t] = w_out[...]

    @pl.when(deputy)
    def _():
        borrowed.wait_recv()
        q = project(other_tokens, 1, lambda i: None)
        first_q[...] = q
        aside(1).start()
        for c in back:
            c.start()

    def wait_w(slot):
        w_copy(w_out, slot, w_send, z, t).wait_recv()

    def wait_mixed(slot):
        send(mixed.at[slot], mixed.at[slot], mx_send, mx_recv.at[slot], z, t).wait_recv()

    def project_out(xx):
        for slot in (2 * xx, 2 * xx + 1):
            pl.when(core != slot % 2)(functools.partial(wait_w, slot))
            pl.when(jnp.logical_and(t != slot, jnp.logical_not(helper)) if slot == 0 else t != slot)(
                functools.partial(wait_mixed, slot)
            )
        pair = jnp.concatenate([mixed[2 * xx], mixed[2 * xx + 1]], axis=1)
        rows = jnp.concatenate([w_all[2 * xx], w_all[2 * xx + 1]], axis=0)
        got = dot(pair, rows)
        if xx == 1 and chips > 1:
            total[...] = got
        elif xx > 0:
            total[...] = total[...] + got
        else:
            out[...] = (total[...] + got if chips > 1 else got).astype(BF16)

    def pass_on():
        for d in range(1, chips):

            @pl.when(jnp.logical_not(outset))
            def _():
                w_copy(w_out, across(d), w_send, z, t).wait_recv()

            @pl.when(jnp.logical_not(jnp.logical_and(first, x == 0)))
            def _():
                passed[d - 1].start()

    early = jnp.logical_and(lead, jnp.logical_and(z >= 1, z <= most))

    @pl.when(jnp.logical_and(jnp.logical_and(core == 1, forwarded > 0), jnp.logical_not(helper)))
    def _():
        aside(0).wait_recv()
        for c in up(0):
            c.start()

    @pl.when(jnp.logical_not(outset))
    def _():
        attend(queries, 0, True)

    def absorb(k, carry):
        beside = jnp.logical_and(z == 1, t == 1)

        @pl.when(jnp.logical_and(core == 1, jnp.logical_not(beside)))
        def _():
            for c in range(len(CHUNKS)):
                up(k - 1)[c].wait_recv()

                @pl.when(k < forwarded)
                def _():
                    up(k)[c].start()

            down(k).start()

        @pl.when(beside)
        def _():
            alone.wait_recv()
            aside(1).wait_recv()

            @pl.when(k < forwarded)
            def _():
                for c in up(1):
                    c.start()

        @pl.when(jnp.logical_and(core == 0, jnp.logical_not(deputy)))
        def _():
            down(k).wait_recv()

        reaches_first = jnp.logical_and(lead, k == z)

        @pl.when(reaches_first)
        def _():
            pass_on()
            for xx in range(1, chips):
                project_out(xx)
            late_rates[0].wait_recv()
            rate_now[...] = late_rate[...].astype(F32)

        @pl.when(jnp.logical_not(reaches_first))
        def _():
            slab_rate(k)

        @pl.when(k <= far)
        def _():
            attend(queries, k, False)

        return carry

    lax.fori_loop(1, received + 1, absorb, 0)

    @pl.when(guest)
    def _():
        answer.wait_recv()
        acc[...] = acc[...] + jnp.exp(-past[...]) * jnp.concatenate([far_got[...].astype(F32)] * 2, axis=0)

    @pl.when(jnp.logical_not(outset))
    def _():
        mixed[t] = join_heads(acc[...]).astype(BF16)

    @pl.when(jnp.logical_not(outset))
    def _():
        for d in sorted(range(1, chips), key=lambda d: -min(d, chips - d)):
            for c in range(2):
                p = 2 * lax.rem(x + d, chips) + c

                @pl.when(jnp.logical_or(z > 0, p != 0))
                def _():
                    mx_copy(p).start()

        @pl.when(jnp.logical_not(helper))
        def _():
            mx_copy(sibling).start()

    pl.when(jnp.logical_not(early))(pass_on)

    @pl.when(jnp.logical_not(jnp.logical_or(outset, early)))
    def _():
        for xx in range(1, chips):
            project_out(xx)

    @pl.when(host)
    def _():
        ask.wait_recv()
        split_heads(far_queries, far_in[...])
        other_acc[...] = jnp.zeros_like(other_acc)
        other_past[...] = jnp.zeros_like(other_past)

        def absorb_far(k, carry):
            reaches_first = jnp.logical_and(lead, k == z)

            @pl.when(reaches_first)
            def _():
                rate_now[...] = late_rate[...].astype(F32)

            @pl.when(jnp.logical_not(reaches_first))
            def _():
                slab_rate(k)

            attend(far_queries, k, False, other_acc, other_past)
            return carry

        lax.fori_loop(1, z + 1, absorb_far, 0)
        far_back[...] = join_heads(other_acc[...]).astype(BF16)
        answer.start()

    @pl.when(helper)
    def _():
        for c in back:
            c.wait_recv()
        split_heads(first_queries, first_q[...])
        late_rates[0].wait_recv()
        rate_now[...] = late_rate[...].astype(F32)
        attend(first_queries, 1, True, other_acc, other_past, 0)
        first_mixed[...] = join_heads(other_acc[...]).astype(BF16)
        for p in first_order:
            first_copy(p).start()
        mixed[0] = first_mixed[...]

    @pl.when(jnp.logical_not(outset))
    def _():
        project_out(0)

    handed = send(out, out, out_send, out_recv, z, sibling)

    @pl.when(helper)
    def _():
        pl.semaphore_wait(late_sem, 1)
        handed.start()
        handed.wait_send()

    @pl.when(outset)
    def _():
        handed.wait_recv()

    def left(ref, sem):
        send(ref, ref, sem, out_recv, z, sibling).wait_send()

    @pl.when(outset)
    def _():
        left(rate, lr_send.at[0])
        left(late_span, lr_send.at[1])

    @pl.when(helper)
    def _():
        borrowed.wait_send()
        alone.wait_send()
        if chips > 1:
            left(w_all.at[pl.ds(0, chips - 1)], w_send)
        if ntp > 2:
            left(mixed.at[pl.ds(0, ntp - 2)], first_send)

    carrier = jnp.logical_and(core == 1, jnp.logical_not(helper))
    for n in range(1, most + 1):

        @pl.when(jnp.logical_and(carrier, forwarded == n))
        def _():
            left(kv.at[pl.ds(0, n)], kv_send)

        @pl.when(
            jnp.logical_and(
                jnp.logical_and(core == 1, received == n), jnp.logical_not(jnp.logical_and(z == 1, t == 1))
            )
        )
        def _():
            left(kv.at[pl.ds(0, n), 0], down_send)

    @pl.when(jnp.logical_and(jnp.logical_and(core == 0, jnp.logical_not(outset)), forwarded > 0))
    def _():
        pl.when(deputy)(lambda: left(kv.at[0], kv_send))
        pl.when(jnp.logical_not(deputy))(lambda: left(kv.at[0, 0], kv_send))

    @pl.when(jnp.logical_not(jnp.logical_and(first, x == 0)))
    def _():
        left(w_all.at[pl.ds(0, ntp - 1)], w_send)

    @pl.when(z > 0)
    def _():
        left(mixed.at[pl.ds(0, ntp - 1)], mx_send)

    if ntp > 2:

        @pl.when(jnp.logical_and(first, t != 0))
        def _():
            left(mixed.at[pl.ds(0, ntp - 2)], mx_send)

    @pl.when(deputy)
    def _():
        left(w_all.at[pl.ds(0, chips)], lent_send)
        for c in back:
            c.wait_send()

    @pl.when(guest)
    def _():
        ask.wait_send()

    @pl.when(host)
    def _():
        answer.wait_send()


def on_device(tokens, norm_gain, w_query, w_key, w_value, w_out, key_rate):
    nsp, ntp = lax.axis_size("sp"), lax.axis_size("tp")
    rows, d = tokens.shape
    width = w_query.shape[1]
    far = nsp // 2
    most = max(far, nsp - 1 - far)
    chips = ntp // 2
    dma = pltpu.SemaphoreType.DMA
    vmem = pltpu.VMEM
    return pl.pallas_call(
        functools.partial(layer, nsp, ntp, far),
        out_shape=jax.ShapeDtypeStruct((rows, d), BF16),
        in_specs=[pl.BlockSpec(memory_space=pltpu.VMEM if i in (1, 6) else pltpu.HBM) for i in range(7)],
        out_specs=pl.BlockSpec(memory_space=pltpu.VMEM),
        scratch_shapes=[
            vmem((rows, d), BF16),
            vmem((d, width), BF16),
            vmem((d, width), BF16),
            vmem((d, width), BF16),
            vmem((width, d), BF16),
            vmem((most + 1, 2, 2 * SPAN + PAD, width), BF16),
            vmem((rows, d), BF16),
            vmem((rows, d), BF16),
            vmem((2 * rows, width), BF16),
            vmem((rows, width), BF16),
            vmem((2 * rows, width), BF16),
            vmem((rows, width), BF16),
            vmem((rows, width), BF16),
            vmem((2 * rows, width), BF16),
            vmem((rows, width), BF16),
            vmem((rows, width), BF16),
            vmem((2 * SPAN, 2 * SPAN), BF16),
            vmem((2, SPAN), F32),
            vmem((2, SPAN), BF16),
            vmem((most, 2, SPAN), BF16),
            vmem((2 * rows, width), F32),
            vmem((2 * rows, SPAN), F32),
            vmem((2 * rows, width), F32),
            vmem((2 * rows, SPAN), F32),
            vmem((ntp, rows, width), BF16),
            vmem((rows, width), BF16),
            vmem((ntp, width, d), BF16),
            vmem((rows, d), F32),
            pltpu.SemaphoreType.REGULAR,
            dma((5,)),
            dma,
            dma((most + 1, len(CHUNKS))),
            dma,
            dma,
            dma,
            dma((ntp,)),
            dma,
            dma,
            dma((ntp,)),
            dma,
            dma,
            dma((2,)),
            dma,
            dma((2,)),
            dma((2,)),
            dma,
            dma,
            dma,
            dma,
            dma,
            dma,
        ],
        compiler_params=pltpu.CompilerParams(
            collective_id=0, has_side_effects=True, vmem_limit_bytes=55_650_000
        ),
    )(tokens, norm_gain.reshape(1, d), w_query, w_key, w_value, w_out, key_rate)


def solution(mesh):
    return jax.shard_map(
        on_device,
        mesh=mesh,
        in_specs=(
            P(("grp", "sp"), None),
            P(),
            P(None, "tp"),
            P(None, "tp"),
            P(None, "tp"),
            P("tp", None),
            P("tp", ("grp", "sp")),
        ),
        out_specs=P(("grp", "sp"), None),
        check_vma=False,
    )
```

```python
import functools

import jax
import jax.numpy as jnp
from jax import lax
from jax.experimental import pallas as pl
from jax.experimental.pallas import tpu as pltpu
from jax.sharding import PartitionSpec as P

HD = 64
SPAN = 128
PAD = 16
VAL = SPAN + PAD
CHUNKS = ((0, 96), (96, 80), (176, 96))

F32 = jnp.float32
BF16 = jnp.bfloat16
EPS = 1e-06
SKIP = 3
MESH = pl.DeviceIdType.MESH


def dot(a, b):
    return lax.dot_general(a, b, (((1,), (0,)), ((), ())), preferred_element_type=F32)


def dot_t(a, b):
    return lax.dot_general(a, b, (((1,), (1,)), ((), ())), preferred_element_type=F32)


def layer(
    nsp,
    ntp,
    far,
    alone_to,
    tokens_hbm,
    gain,
    w_query_hbm,
    w_key_hbm,
    w_value_hbm,
    w_out_hbm,
    rate,
    out,
    tokens,
    w_query,
    w_key,
    w_value,
    w_out,
    kv,
    normed,
    other_tokens,
    queries,
    first_q,
    first_queries,
    far_sent,
    far_in,
    far_queries,
    far_back,
    far_got,
    tri,
    rate_now,
    late_rate,
    late_span,
    acc,
    past,
    other_acc,
    other_past,
    mixed,
    first_mixed,
    w_all,
    total,
    late_sem,
    ready_sem,
    load,
    kv_send,
    kv_recv,
    down_send,
    w_send,
    lent_send,
    w_recv,
    mx_send,
    first_send,
    mx_recv,
    tok_send,
    tok_recv,
    lr_send,
    lr_recv,
    relay_send,
    h_send,
    h_recv,
    fq_send,
    fq_recv,
    fa_send,
    fa_recv,
    out_send,
    out_recv,
):
    z = lax.axis_index("sp")
    t = lax.axis_index("tp")
    chips = ntp // 2
    x, core = t // 2, lax.rem(t, 2)
    sibling = 2 * x + 1 - core
    reach = nsp - 1 - far
    most = max(alone_to, reach)
    near = min(nsp // 4, most)
    lead = t == 0
    first = z == 0
    last = z == nsp - 1
    outset = jnp.logical_and(first, lead)
    deputy = jnp.logical_and(z == 1, lead)
    helper = jnp.logical_and(first, t == 1)
    host = jnp.logical_and(z > alone_to - far, z <= reach)
    guest = z > alone_to

    bar = pltpu.get_barrier_semaphore()

    def at(zz, tt):
        return {"sp": zz, "tp": tt}

    def greet(zz, tt):
        pl.semaphore_signal(bar, inc=1, device_id=at(zz, tt), device_id_type=MESH)

    def send(src, dst, ss, rs, zz, tt):
        return pltpu.make_async_remote_copy(
            src_ref=src, dst_ref=dst, send_sem=ss, recv_sem=rs, device_id=at(zz, tt), device_id_type=MESH
        )

    loads = [
        pltpu.make_async_copy(a, b, load.at[i])
        for i, (a, b) in enumerate(
            (
                (tokens_hbm, tokens),
                (w_query_hbm, w_query),
                (w_key_hbm, w_key),
                (w_value_hbm, w_value),
                (w_out_hbm, w_out),
            )
        )
    ]

    @pl.when(jnp.logical_not(outset))
    def _():
        for c in loads:
            c.start()

    @pl.when(jnp.logical_and(z >= 1, core == 1))
    def _():
        greet(z - 1, t)

    for p in range(ntp):

        @pl.when(jnp.logical_and(t != 0, t != p))
        def _():
            greet(z, p)

    @pl.when(host)
    def _():
        greet(z + far, t)

    @pl.when(jnp.logical_and(jnp.logical_and(z >= 1, z <= near), lead))
    def _():
        greet(0, 0)

    @pl.when(jnp.logical_and(first, t != 0))
    def _():
        greet(1, 0)

    @pl.when(deputy)
    def _():
        greet(0, 1)

    one = lambda flag: jnp.where(flag, 1, 0)
    expected = (
        one(jnp.logical_and(jnp.logical_not(last), core == 1))
        + jnp.where(lead, ntp - 1, ntp - 2)
        + one(guest)
        + one(outset) * near
        + one(deputy) * (ntp - 1)
        + one(helper)
    )

    late_rates = [send(rate, late_rate, lr_send.at[0], lr_recv, 0, 1)] + [
        send(rate, late_rate, lr_send.at[1], lr_recv, i, 0) for i in range(1, near + 1)
    ]

    @pl.when(outset)
    def _():
        pl.semaphore_wait(bar, expected)
        for c in late_rates:
            c.start()

    @pl.when(jnp.logical_not(outset))
    def _():
        row = lax.broadcasted_iota(jnp.int32, (2 * SPAN, 2 * SPAN), 0)
        col = lax.broadcasted_iota(jnp.int32, (2 * SPAN, 2 * SPAN), 1)
        later = jnp.logical_or(col >= SPAN, lax.rem(row, SPAN) >= col)
        tri[...] = jnp.where(later, 1.0, 0.0).astype(BF16)

    def split_heads(dst, q):
        lane = lax.broadcasted_iota(jnp.int32, (SPAN, 2 * HD), 1)
        qf = q.astype(F32)
        dst[:SPAN] = jnp.where(lane < HD, qf, 0.0).astype(BF16)
        dst[SPAN:] = jnp.where(lane >= HD, qf, 0.0).astype(BF16)

    def join_heads(a):
        lane = lax.broadcasted_iota(jnp.int32, (SPAN, 2 * HD), 1)
        return jnp.where(lane < HD, a[:SPAN], a[SPAN:])

    def project_queries(src, wait):
        wait(0)
        xs = src[...].astype(F32)
        scale = lax.rsqrt(jnp.mean(xs * xs, axis=-1, keepdims=True) + EPS)
        normed[...] = (xs * scale * gain[...]).astype(BF16)
        wait(1)
        return dot(normed[...], w_query[...]).astype(BF16) * HD ** (-0.5)

    def project_slab(slot, wait):
        wait(2)
        kv[slot, core, pl.ds(0, SPAN)] = dot(normed[...], w_key[...]).astype(BF16)
        wait(3)
        kv[slot, core, pl.ds(VAL, SPAN)] = dot(normed[...], w_value[...]).astype(BF16)
        kv[slot, core, pl.ds(SPAN, PAD)] = jnp.concatenate(
            [rate[...].astype(F32), jnp.zeros((PAD - 2, SPAN), F32)], axis=0
        ).astype(BF16)

    def attend(q_ref, slot, diagonal, acc=acc, past=past, part=core):
        s = dot_t(q_ref[...], kv[slot, part, pl.ds(0, SPAN)])
        s = jnp.concatenate([s[:SPAN] + rate_now[0:1], s[SPAN:] + rate_now[1:2]], axis=0)
        soft = jnp.maximum(s, 0.0) + jnp.log(1.0 + jnp.exp(-jnp.abs(s)))
        if diagonal:
            r = lax.rem(lax.broadcasted_iota(jnp.int32, (2 * SPAN, SPAN), 0), SPAN)
            c = lax.broadcasted_iota(jnp.int32, (2 * SPAN, SPAN), 1)
            seen = c < r
            soft = jnp.where(seen, soft, 0.0)
        high = soft.astype(BF16)
        low = (soft - high.astype(F32)).astype(BF16)
        sums = dot(jnp.concatenate([high, low], axis=1), tri[...])
        weight = jnp.exp(s - sums[:, :SPAN])
        if diagonal:
            weight = jnp.where(seen, weight, 0.0)
        got = dot(weight.astype(BF16), kv[slot, part, pl.ds(VAL, SPAN)])
        if diagonal:
            acc[...] = got
            past[...] = sums[:, SPAN:]
        else:
            acc[...] = acc[...] + jnp.exp(-past[...]) * got
            past[...] = past[...] + sums[:, SPAN:]

    def slab_rate(slot):
        rate_now[...] = kv[slot, core, pl.ds(SPAN, PAD)][:2].astype(F32)

    ask = send(far_sent, far_in, fq_send, fq_recv, z - far, t)
    answer = send(far_back, far_got, fa_send, fa_recv, z + far, t)

    @pl.when(jnp.logical_not(outset))
    def _():
        q = project_queries(tokens, lambda i: loads[i].wait())
        far_sent[...] = q
        split_heads(queries, q)
        pl.semaphore_wait(bar, expected)

        @pl.when(guest)
        def _():
            ask.start()

        project_slab(0, lambda i: loads[i].wait())
        slab_rate(0)
        loads[4].wait()

    borrowed = send(tokens, other_tokens, tok_send, tok_recv, 1, 0)

    def w_copy(src, slot, sem, zz, tt):
        return send(src, w_all.at[slot], sem, w_recv.at[slot], zz, tt)

    def across(d):
        return 2 * lax.rem(x + d, chips) + core

    directs = [w_copy(w_out, t, w_send, z, across(d)) for d in range(1, chips)]
    to_sibling = w_copy(w_out, t, w_send, z, sibling)
    passed = [w_copy(w_all.at[across(d)], across(d), w_send, z, sibling) for d in range(1, chips)]
    lent = [w_copy(w_out, 0, lent_send, 0, p) for p in [1] + list(range(2, ntp, 2))]
    to_helper = w_copy(w_out, t, w_send, 0, 1)

    def up(k):
        return [
            send(kv.at[k, :, pl.ds(a, n)], kv.at[k + 1, :, pl.ds(a, n)], kv_send, kv_recv.at[k + 1, c], z + 1, t)
            for c, (a, n) in enumerate(CHUNKS)
        ]

    def down(k):
        return send(kv.at[k, 0], kv.at[k, 0], down_send, kv_recv.at[k, 0], z, sibling)

    def aside(k):
        return send(kv.at[k, 0], kv.at[k, 0], kv_send, kv_recv.at[k, 0], z, sibling)

    alone = send(kv.at[0, 1], kv.at[1, 1], kv_send, kv_recv.at[1, 1], 1, 1)
    back = [
        send(kv.at[1, 0], kv.at[1, 0], h_send.at[0], h_recv.at[0], 0, 1),
        send(first_q, first_q, h_send.at[1], h_recv.at[1], 0, 1),
    ]

    def mx_copy(p):
        return send(mixed.at[t], mixed.at[t], mx_send, mx_recv.at[t], z, p)

    def first_copy(p):
        return send(first_mixed, mixed.at[0], first_send, mx_recv.at[0], 0, p)

    first_order = list(range(4, min(6, ntp))) + [p for p in range(2, ntp) if p not in (4, 5)]

    def needed(zz):
        return jnp.where(zz <= most, zz, far)

    received = needed(z)
    forwarded = jnp.where(last, 0, needed(z + 1))

    @pl.when(helper)
    def _():
        borrowed.start()

    @pl.when(helper)
    def _():
        alone.start()

    @pl.when(jnp.logical_and(jnp.logical_and(core == 0, jnp.logical_not(outset)), forwarded > 0))
    def _():
        aside(0).start()

    for p in range(1, ntp):

        @pl.when(jnp.logical_and(lead, z > 0) if p > 1 else lead)
        def _():
            pl.semaphore_signal(late_sem, inc=1, device_id=at(z, p), device_id_type=MESH)

    @pl.when(jnp.logical_not(outset))
    def _():
        for d in range(1, chips):

            @pl.when(across(d) != 0)
            def _():
                directs[d - 1].start()

        @pl.when(sibling != 0)
        def _():
            to_sibling.start()

    @pl.when(deputy)
    def _():
        for c in lent:
            c.start()

    @pl.when(jnp.logical_and(first, jnp.logical_and(core == 0, t != 0)))
    def _():
        to_helper.start()

    def to_lead():
        pl.semaphore_wait(late_sem, 1)
        for d in range(1, chips):

            @pl.when(across(d) == 0)
            def _():
                directs[d - 1].start()

        @pl.when(sibling == 0)
        def _():
            to_sibling.start()

    @pl.when(jnp.logical_and(z > 0, t != 0))
    def _():
        to_lead()

    @pl.when(jnp.logical_not(outset))
    def _():
        w_all[t] = w_out[...]

    @pl.when(deputy)
    def _():
        borrowed.wait_recv()
        first_q[...] = project_queries(other_tokens, lambda i: None)
        project_slab(1, lambda i: None)
        aside(1).start()
        for c in back:
            c.start()

    def wait_w(slot):
        w_copy(w_out, slot, w_send, z, t).wait_recv()

    def wait_mixed(slot):
        send(mixed.at[slot], mixed.at[slot], mx_send, mx_recv.at[slot], z, t).wait_recv()

    def project_out(xx):
        for slot in (2 * xx, 2 * xx + 1):
            pl.when(core != slot % 2)(functools.partial(wait_w, slot))
            pl.when(jnp.logical_and(t != slot, jnp.logical_not(helper)) if slot == 0 else t != slot)(
                functools.partial(wait_mixed, slot)
            )
        pair = jnp.concatenate([mixed[2 * xx], mixed[2 * xx + 1]], axis=1)
        rows = jnp.concatenate([w_all[2 * xx], w_all[2 * xx + 1]], axis=0)
        got = dot(pair, rows)
        if xx == 1 and chips > 1:
            total[...] = got
        elif xx > 0:
            total[...] = total[...] + got
        else:
            out[...] = (total[...] + got if chips > 1 else got).astype(BF16)

    def pass_on():
        for d in range(1, chips):

            @pl.when(jnp.logical_not(outset))
            def _():
                w_copy(w_out, across(d), w_send, z, t).wait_recv()

            @pl.when(jnp.logical_not(jnp.logical_and(first, x == 0)))
            def _():
                passed[d - 1].start()

    early = jnp.logical_and(lead, jnp.logical_and(z >= 1, z <= reach // 2))

    relays = jnp.logical_and(lead, jnp.logical_and(z >= 1, z <= most - near))
    relayed = send(late_rate, late_rate, relay_send, lr_recv, z + near, 0)

    def relay():
        pl.semaphore_wait(ready_sem, 1)
        relayed.start()

    @pl.when(jnp.logical_and(jnp.logical_and(core == 1, forwarded > 0), jnp.logical_not(helper)))
    def _():
        aside(0).wait_recv()
        for c in up(0):
            c.start()

    @pl.when(jnp.logical_not(outset))
    def _():
        attend(queries, 0, True)

    def absorb(k, carry):
        beside = jnp.logical_and(z == 1, t == 1)

        @pl.when(jnp.logical_and(core == 1, jnp.logical_not(beside)))
        def _():
            for c in range(len(CHUNKS)):
                up(k - 1)[c].wait_recv()

                @pl.when(k < forwarded)
                def _():
                    up(k)[c].start()

            down(k).start()

        @pl.when(beside)
        def _():
            alone.wait_recv()
            aside(1).wait_recv()

            @pl.when(k < forwarded)
            def _():
                for c in up(1):
                    c.start()

        @pl.when(jnp.logical_and(core == 0, jnp.logical_not(deputy)))
        def _():
            down(k).wait_recv()

            @pl.when(jnp.logical_and(jnp.logical_and(lead, k == near), jnp.logical_and(z > near, z <= most)))
            def _():
                pl.semaphore_signal(ready_sem, inc=1, device_id=at(z - near, 0), device_id_type=MESH)

        reaches_first = jnp.logical_and(lead, k == z)

        @pl.when(reaches_first)
        def _():
            @pl.when(early)
            def _():
                pass_on()
                for xx in range(1, chips):
                    project_out(xx)

            late_rates[0].wait_recv()
            pl.when(jnp.logical_and(relays, z < near // 2))(relay)
            rate_now[...] = late_rate[...].astype(F32)

        @pl.when(jnp.logical_not(reaches_first))
        def _():
            slab_rate(k)

        @pl.when(jnp.logical_or(k <= far, z <= alone_to))
        def _():
            attend(queries, k, False)

        return carry

    lax.fori_loop(1, received + 1, absorb, 0)

    @pl.when(guest)
    def _():
        answer.wait_recv()
        acc[...] = acc[...] + jnp.exp(-past[...]) * jnp.concatenate([far_got[...].astype(F32)] * 2, axis=0)

    @pl.when(jnp.logical_not(outset))
    def _():
        mixed[t] = join_heads(acc[...]).astype(BF16)

    @pl.when(jnp.logical_not(outset))
    def _():
        for d in sorted(range(1, chips), key=lambda d: -min(d, chips - d)):
            for c in range(2):
                p = 2 * lax.rem(x + d, chips) + c

                @pl.when(jnp.logical_or(z > 0, p != 0))
                def _():
                    mx_copy(p).start()

        @pl.when(jnp.logical_not(helper))
        def _():
            mx_copy(sibling).start()

    pl.when(jnp.logical_not(early))(pass_on)

    def serve():
        ask.wait_recv()
        split_heads(far_queries, far_in[...])
        other_acc[...] = jnp.zeros_like(other_acc)
        other_past[...] = jnp.zeros_like(other_past)

        def absorb_far(k, carry):
            reaches_first = jnp.logical_and(lead, k == z)

            @pl.when(reaches_first)
            def _():
                rate_now[...] = late_rate[...].astype(F32)

            @pl.when(jnp.logical_not(reaches_first))
            def _():
                slab_rate(k)

            attend(far_queries, k, False, other_acc, other_past)
            return carry

        lax.fori_loop(1, z + 1, absorb_far, 0)
        far_back[...] = join_heads(other_acc[...]).astype(BF16)
        answer.start()

    soon = z > reach // 2
    pl.when(jnp.logical_and(host, soon))(serve)
    pl.when(jnp.logical_and(relays, z >= near // 2))(relay)

    @pl.when(jnp.logical_not(jnp.logical_or(outset, early)))
    def _():
        for xx in range(1, chips):
            project_out(xx)

    pl.when(jnp.logical_and(host, jnp.logical_not(soon)))(serve)

    @pl.when(helper)
    def _():
        for c in back:
            c.wait_recv()
        split_heads(first_queries, first_q[...])
        late_rates[0].wait_recv()
        rate_now[...] = late_rate[...].astype(F32)
        attend(first_queries, 1, True, other_acc, other_past, 0)
        first_mixed[...] = join_heads(other_acc[...]).astype(BF16)
        for p in first_order:
            first_copy(p).start()
        mixed[0] = first_mixed[...]

    @pl.when(jnp.logical_not(outset))
    def _():
        project_out(0)

    handed = send(out, out, out_send, out_recv, z, sibling)

    @pl.when(helper)
    def _():
        pl.semaphore_wait(late_sem, 1)
        handed.start()
        handed.wait_send()

    @pl.when(outset)
    def _():
        handed.wait_recv()

    def left(ref, sem):
        send(ref, ref, sem, out_recv, z, sibling).wait_send()

    @pl.when(outset)
    def _():
        left(rate, lr_send.at[0])
        left(late_span, lr_send.at[1])

    @pl.when(helper)
    def _():
        borrowed.wait_send()
        alone.wait_send()
        if chips > 1:
            left(w_all.at[pl.ds(0, chips - 1)], w_send)
        if ntp > 2:
            left(mixed.at[pl.ds(0, ntp - 2)], first_send)

    carrier = jnp.logical_and(core == 1, jnp.logical_not(helper))
    for n in range(1, most + 1):

        @pl.when(jnp.logical_and(carrier, forwarded == n))
        def _():
            left(kv.at[pl.ds(0, n)], kv_send)

        @pl.when(
            jnp.logical_and(
                jnp.logical_and(core == 1, received == n), jnp.logical_not(jnp.logical_and(z == 1, t == 1))
            )
        )
        def _():
            left(kv.at[pl.ds(0, n), 0], down_send)

    @pl.when(jnp.logical_and(jnp.logical_and(core == 0, jnp.logical_not(outset)), forwarded > 0))
    def _():
        pl.when(deputy)(lambda: left(kv.at[0], kv_send))
        pl.when(jnp.logical_not(deputy))(lambda: left(kv.at[0, 0], kv_send))

    @pl.when(jnp.logical_not(jnp.logical_and(first, x == 0)))
    def _():
        left(w_all.at[pl.ds(0, ntp - 1)], w_send)

    @pl.when(z > 0)
    def _():
        left(mixed.at[pl.ds(0, ntp - 1)], mx_send)

    if ntp > 2:

        @pl.when(jnp.logical_and(first, t != 0))
        def _():
            left(mixed.at[pl.ds(0, ntp - 2)], mx_send)

    @pl.when(deputy)
    def _():
        left(w_all.at[pl.ds(0, chips)], lent_send)
        for c in back:
            c.wait_send()

    @pl.when(relays)
    def _():
        relayed.wait_send()

    @pl.when(guest)
    def _():
        ask.wait_send()

    @pl.when(host)
    def _():
        answer.wait_send()


def on_device(tokens, norm_gain, w_query, w_key, w_value, w_out, key_rate):
    nsp, ntp = lax.axis_size("sp"), lax.axis_size("tp")
    rows, d = tokens.shape
    width = w_query.shape[1]
    far = nsp // 2
    alone_to = min(far + SKIP, nsp - 1)
    most = max(alone_to, nsp - 1 - far)
    chips = ntp // 2
    dma = pltpu.SemaphoreType.DMA
    vmem = pltpu.VMEM
    return pl.pallas_call(
        functools.partial(layer, nsp, ntp, far, alone_to),
        out_shape=jax.ShapeDtypeStruct((rows, d), BF16),
        in_specs=[pl.BlockSpec(memory_space=pltpu.VMEM if i in (1, 6) else pltpu.HBM) for i in range(7)],
        out_specs=pl.BlockSpec(memory_space=pltpu.VMEM),
        scratch_shapes=[
            vmem((rows, d), BF16),
            vmem((d, width), BF16),
            vmem((d, width), BF16),
            vmem((d, width), BF16),
            vmem((width, d), BF16),
            vmem((most + 1, 2, 2 * SPAN + PAD, width), BF16),
            vmem((rows, d), BF16),
            vmem((rows, d), BF16),
            vmem((2 * rows, width), BF16),
            vmem((rows, width), BF16),
            vmem((2 * rows, width), BF16),
            vmem((rows, width), BF16),
            vmem((rows, width), BF16),
            vmem((2 * rows, width), BF16),
            vmem((rows, width), BF16),
            vmem((rows, width), BF16),
            vmem((2 * SPAN, 2 * SPAN), BF16),
            vmem((2, SPAN), F32),
            vmem((2, SPAN), BF16),
            vmem((min(nsp // 4, most), 2, SPAN), BF16),
            vmem((2 * rows, width), F32),
            vmem((2 * rows, SPAN), F32),
            vmem((2 * rows, width), F32),
            vmem((2 * rows, SPAN), F32),
            vmem((ntp, rows, width), BF16),
            vmem((rows, width), BF16),
            vmem((ntp, width, d), BF16),
            vmem((rows, d), F32),
            pltpu.SemaphoreType.REGULAR,
            pltpu.SemaphoreType.REGULAR,
            dma((5,)),
            dma,
            dma((most + 1, len(CHUNKS))),
            dma,
            dma,
            dma,
            dma((ntp,)),
            dma,
            dma,
            dma((ntp,)),
            dma,
            dma,
            dma((2,)),
            dma,
            dma,
            dma((2,)),
            dma((2,)),
            dma,
            dma,
            dma,
            dma,
            dma,
            dma,
        ],
        compiler_params=pltpu.CompilerParams(
            collective_id=0, has_side_effects=True, vmem_limit_bytes=55_650_000
        ),
    )(tokens, norm_gain.reshape(1, d), w_query, w_key, w_value, w_out, key_rate)


def solution(mesh):
    return jax.shard_map(
        on_device,
        mesh=mesh,
        in_specs=(
            P(("grp", "sp"), None),
            P(),
            P(None, "tp"),
            P(None, "tp"),
            P(None, "tp"),
            P("tp", None),
            P("tp", ("grp", "sp")),
        ),
        out_specs=P(("grp", "sp"), None),
        check_vma=False,
    )
```

```python
import functools

import jax
import jax.numpy as jnp
from jax import lax
from jax.experimental import pallas as pl
from jax.experimental.pallas import tpu as pltpu
from jax.sharding import PartitionSpec as P

HD = 64
SPAN = 128
PAD = 16
VAL = SPAN + PAD
CHUNKS = ((0, 96), (96, 80), (176, 96))

F32 = jnp.float32
BF16 = jnp.bfloat16
EPS = 1e-06
SKIP = 3
MESH = pl.DeviceIdType.MESH


def dot(a, b):
    return lax.dot_general(a, b, (((1,), (0,)), ((), ())), preferred_element_type=F32)


def dot_t(a, b):
    return lax.dot_general(a, b, (((1,), (1,)), ((), ())), preferred_element_type=F32)


def layer(
    nsp,
    ntp,
    far,
    alone_to,
    tokens_hbm,
    gain,
    w_query_hbm,
    w_key_hbm,
    w_value_hbm,
    w_out_hbm,
    rate,
    out,
    tokens,
    w_query,
    w_key,
    w_value,
    w_out,
    kv,
    normed,
    other_tokens,
    queries,
    first_q,
    first_queries,
    far_sent,
    far_in,
    far_queries,
    far_back,
    far_got,
    tri,
    rate_now,
    late_rate,
    late_span,
    acc,
    past,
    other_acc,
    other_past,
    mixed,
    first_mixed,
    w_all,
    total,
    late_sem,
    ready_sem,
    load,
    kv_send,
    kv_recv,
    down_send,
    w_send,
    lent_send,
    w_recv,
    mx_send,
    first_send,
    mx_recv,
    tok_send,
    tok_recv,
    lr_send,
    lr_recv,
    relay_send,
    h_send,
    h_recv,
    fq_send,
    fq_recv,
    fa_send,
    fa_recv,
    out_send,
    out_recv,
):
    z = lax.axis_index("sp")
    t = lax.axis_index("tp")
    chips = ntp // 2
    x, core = t // 2, lax.rem(t, 2)
    sibling = 2 * x + 1 - core
    reach = nsp - 1 - far
    most = max(alone_to, reach)
    near = min(nsp // 4, most)
    lead = t == 0
    first = z == 0
    last = z == nsp - 1
    outset = jnp.logical_and(first, lead)
    deputy = jnp.logical_and(z == 1, lead)
    helper = jnp.logical_and(first, t == 1)
    host = jnp.logical_and(z > alone_to - far, z <= reach)
    guest = z > alone_to

    bar = pltpu.get_barrier_semaphore()

    def at(zz, tt):
        return {"sp": zz, "tp": tt}

    def greet(zz, tt):
        pl.semaphore_signal(bar, inc=1, device_id=at(zz, tt), device_id_type=MESH)

    def send(src, dst, ss, rs, zz, tt):
        return pltpu.make_async_remote_copy(
            src_ref=src, dst_ref=dst, send_sem=ss, recv_sem=rs, device_id=at(zz, tt), device_id_type=MESH
        )

    loads = [
        pltpu.make_async_copy(a, b, load.at[i])
        for i, (a, b) in enumerate(
            (
                (tokens_hbm, tokens),
                (w_query_hbm, w_query),
                (w_key_hbm, w_key),
                (w_value_hbm, w_value),
                (w_out_hbm, w_out),
            )
        )
    ]

    @pl.when(jnp.logical_not(outset))
    def _():
        for c in loads:
            c.start()

    @pl.when(jnp.logical_and(z >= 1, core == 1))
    def _():
        greet(z - 1, t)

    for p in range(ntp):

        @pl.when(jnp.logical_and(t != 0, t != p))
        def _():
            greet(z, p)

    @pl.when(host)
    def _():
        greet(z + far, t)

    @pl.when(jnp.logical_and(jnp.logical_and(z >= 1, z <= near), lead))
    def _():
        greet(0, 0)

    @pl.when(jnp.logical_and(first, t != 0))
    def _():
        greet(1, 0)

    @pl.when(deputy)
    def _():
        greet(0, 1)

    one = lambda flag: jnp.where(flag, 1, 0)
    expected = (
        one(jnp.logical_and(jnp.logical_not(last), core == 1))
        + jnp.where(lead, ntp - 1, ntp - 2)
        + one(guest)
        + one(outset) * near
        + one(deputy) * (ntp - 1)
        + one(helper)
    )

    late_rates = [send(rate, late_rate, lr_send.at[0], lr_recv, 0, 1)] + [
        send(rate, late_rate, lr_send.at[1], lr_recv, i, 0) for i in range(1, near + 1)
    ]

    @pl.when(outset)
    def _():
        pl.semaphore_wait(bar, expected)
        for c in late_rates:
            c.start()

    @pl.when(jnp.logical_not(outset))
    def _():
        row = lax.broadcasted_iota(jnp.int32, (2 * SPAN, 2 * SPAN), 0)
        col = lax.broadcasted_iota(jnp.int32, (2 * SPAN, 2 * SPAN), 1)
        later = jnp.logical_or(col >= SPAN, lax.rem(row, SPAN) >= col)
        tri[...] = jnp.where(later, 1.0, 0.0).astype(BF16)

    def split_heads(dst, q):
        lane = lax.broadcasted_iota(jnp.int32, (SPAN, 2 * HD), 1)
        qf = q.astype(F32)
        dst[:SPAN] = jnp.where(lane < HD, qf, 0.0).astype(BF16)
        dst[SPAN:] = jnp.where(lane >= HD, qf, 0.0).astype(BF16)

    def join_heads(a):
        lane = lax.broadcasted_iota(jnp.int32, (SPAN, 2 * HD), 1)
        return jnp.where(lane < HD, a[:SPAN], a[SPAN:])

    def project_queries(src, wait):
        wait(0)
        xs = src[...].astype(F32)
        scale = lax.rsqrt(jnp.mean(xs * xs, axis=-1, keepdims=True) + EPS)
        normed[...] = (xs * scale * gain[...]).astype(BF16)
        wait(1)
        return dot(normed[...], w_query[...]).astype(BF16) * HD ** (-0.5)

    def project_slab(slot, wait):
        wait(2)
        kv[slot, core, pl.ds(0, SPAN)] = dot(normed[...], w_key[...]).astype(BF16)
        wait(3)
        kv[slot, core, pl.ds(VAL, SPAN)] = dot(normed[...], w_value[...]).astype(BF16)
        kv[slot, core, pl.ds(SPAN, PAD)] = jnp.concatenate(
            [rate[...].astype(F32), jnp.zeros((PAD - 2, SPAN), F32)], axis=0
        ).astype(BF16)

    def attend(q_ref, slot, diagonal, acc=acc, past=past, part=core):
        s = dot_t(q_ref[...], kv[slot, part, pl.ds(0, SPAN)])
        s = jnp.concatenate([s[:SPAN] + rate_now[0:1], s[SPAN:] + rate_now[1:2]], axis=0)
        soft = jnp.maximum(s, 0.0) + jnp.log(1.0 + jnp.exp(-jnp.abs(s)))
        if diagonal:
            r = lax.rem(lax.broadcasted_iota(jnp.int32, (2 * SPAN, SPAN), 0), SPAN)
            c = lax.broadcasted_iota(jnp.int32, (2 * SPAN, SPAN), 1)
            seen = c < r
            soft = jnp.where(seen, soft, 0.0)
        high = soft.astype(BF16)
        low = (soft - high.astype(F32)).astype(BF16)
        sums = dot(jnp.concatenate([high, low], axis=1), tri[...])
        weight = jnp.exp(s - sums[:, :SPAN])
        if diagonal:
            weight = jnp.where(seen, weight, 0.0)
        got = dot(weight.astype(BF16), kv[slot, part, pl.ds(VAL, SPAN)])
        if diagonal:
            acc[...] = got
            past[...] = sums[:, SPAN:]
        else:
            acc[...] = acc[...] + jnp.exp(-past[...]) * got
            past[...] = past[...] + sums[:, SPAN:]

    def slab_rate(slot):
        rate_now[...] = kv[slot, core, pl.ds(SPAN, PAD)][:2].astype(F32)

    ask = send(far_sent, far_in, fq_send, fq_recv, z - far, t)
    answer = send(far_back, far_got, fa_send, fa_recv, z + far, t)

    @pl.when(jnp.logical_not(outset))
    def _():
        q = project_queries(tokens, lambda i: loads[i].wait())
        far_sent[...] = q
        split_heads(queries, q)

        @pl.when(jnp.logical_not(guest))
        def _():
            project_slab(0, lambda i: loads[i].wait())

        pl.semaphore_wait(bar, expected)

        @pl.when(guest)
        def _():
            ask.start()
            project_slab(0, lambda i: loads[i].wait())

        slab_rate(0)
        loads[4].wait()

    borrowed = send(tokens, other_tokens, tok_send, tok_recv, 1, 0)

    def w_copy(src, slot, sem, zz, tt):
        return send(src, w_all.at[slot], sem, w_recv.at[slot], zz, tt)

    def across(d):
        return 2 * lax.rem(x + d, chips) + core

    directs = [w_copy(w_out, t, w_send, z, across(d)) for d in range(1, chips)]
    to_sibling = w_copy(w_out, t, w_send, z, sibling)
    passed = [w_copy(w_all.at[across(d)], across(d), w_send, z, sibling) for d in range(1, chips)]
    lent = [w_copy(w_out, 0, lent_send, 0, p) for p in [1] + list(range(2, ntp, 2))]
    to_helper = w_copy(w_out, t, w_send, 0, 1)

    def up(k):
        return [
            send(kv.at[k, :, pl.ds(a, n)], kv.at[k + 1, :, pl.ds(a, n)], kv_send, kv_recv.at[k + 1, c], z + 1, t)
            for c, (a, n) in enumerate(CHUNKS)
        ]

    def down(k):
        return send(kv.at[k, 0], kv.at[k, 0], down_send, kv_recv.at[k, 0], z, sibling)

    def aside(k):
        return send(kv.at[k, 0], kv.at[k, 0], kv_send, kv_recv.at[k, 0], z, sibling)

    alone = send(kv.at[0, 1], kv.at[1, 1], kv_send, kv_recv.at[1, 1], 1, 1)
    back = [
        send(kv.at[1, 0], kv.at[1, 0], h_send.at[0], h_recv.at[0], 0, 1),
        send(first_q, first_q, h_send.at[1], h_recv.at[1], 0, 1),
    ]

    def mx_copy(p):
        return send(mixed.at[t], mixed.at[t], mx_send, mx_recv.at[t], z, p)

    def first_copy(p):
        return send(first_mixed, mixed.at[0], first_send, mx_recv.at[0], 0, p)

    first_order = list(range(4, min(6, ntp))) + [p for p in range(2, ntp) if p not in (4, 5)]

    def needed(zz):
        return jnp.where(zz <= most, zz, far)

    received = needed(z)
    forwarded = jnp.where(last, 0, needed(z + 1))

    @pl.when(helper)
    def _():
        borrowed.start()

    @pl.when(helper)
    def _():
        alone.start()

    @pl.when(jnp.logical_and(jnp.logical_and(core == 0, jnp.logical_not(outset)), forwarded > 0))
    def _():
        aside(0).start()

    for p in range(1, ntp):

        @pl.when(jnp.logical_and(lead, z > 0) if p > 1 else lead)
        def _():
            pl.semaphore_signal(late_sem, inc=1, device_id=at(z, p), device_id_type=MESH)

    @pl.when(jnp.logical_not(outset))
    def _():
        for d in range(1, chips):

            @pl.when(across(d) != 0)
            def _():
                directs[d - 1].start()

        @pl.when(sibling != 0)
        def _():
            to_sibling.start()

    @pl.when(deputy)
    def _():
        for c in lent:
            c.start()

    @pl.when(jnp.logical_and(first, jnp.logical_and(core == 0, t != 0)))
    def _():
        to_helper.start()

    def to_lead():
        pl.semaphore_wait(late_sem, 1)
        for d in range(1, chips):

            @pl.when(across(d) == 0)
            def _():
                directs[d - 1].start()

        @pl.when(sibling == 0)
        def _():
            to_sibling.start()

    @pl.when(jnp.logical_and(z > 0, t != 0))
    def _():
        to_lead()

    @pl.when(jnp.logical_not(outset))
    def _():
        w_all[t] = w_out[...]

    @pl.when(deputy)
    def _():
        borrowed.wait_recv()
        first_q[...] = project_queries(other_tokens, lambda i: None)
        project_slab(1, lambda i: None)
        aside(1).start()
        for c in back:
            c.start()

    def wait_w(slot):
        w_copy(w_out, slot, w_send, z, t).wait_recv()

    def wait_mixed(slot):
        send(mixed.at[slot], mixed.at[slot], mx_send, mx_recv.at[slot], z, t).wait_recv()

    def project_out(xx):
        for slot in (2 * xx, 2 * xx + 1):
            pl.when(core != slot % 2)(functools.partial(wait_w, slot))
            pl.when(jnp.logical_and(t != slot, jnp.logical_not(helper)) if slot == 0 else t != slot)(
                functools.partial(wait_mixed, slot)
            )
        pair = jnp.concatenate([mixed[2 * xx], mixed[2 * xx + 1]], axis=1)
        rows = jnp.concatenate([w_all[2 * xx], w_all[2 * xx + 1]], axis=0)
        got = dot(pair, rows)
        if xx == 1 and chips > 1:
            total[...] = got
        elif xx > 0:
            total[...] = total[...] + got
        else:
            out[...] = (total[...] + got if chips > 1 else got).astype(BF16)

    def pass_on():
        for d in range(1, chips):

            @pl.when(jnp.logical_not(outset))
            def _():
                w_copy(w_out, across(d), w_send, z, t).wait_recv()

            @pl.when(jnp.logical_not(jnp.logical_and(first, x == 0)))
            def _():
                passed[d - 1].start()

    early = jnp.logical_and(lead, jnp.logical_and(z >= 1, z <= reach // 2))

    relays = jnp.logical_and(lead, jnp.logical_and(z >= 1, z <= most - near))
    relayed = send(late_rate, late_rate, relay_send, lr_recv, z + near, 0)

    def relay():
        pl.semaphore_wait(ready_sem, 1)
        relayed.start()

    @pl.when(jnp.logical_and(jnp.logical_and(core == 1, forwarded > 0), jnp.logical_not(helper)))
    def _():
        aside(0).wait_recv()
        for c in up(0):
            c.start()

    @pl.when(jnp.logical_not(outset))
    def _():
        attend(queries, 0, True)

    def absorb(k, carry):
        beside = jnp.logical_and(z == 1, t == 1)

        @pl.when(jnp.logical_and(core == 1, jnp.logical_not(beside)))
        def _():
            for c in range(len(CHUNKS)):
                up(k - 1)[c].wait_recv()

                @pl.when(k < forwarded)
                def _():
                    up(k)[c].start()

            down(k).start()

        @pl.when(beside)
        def _():
            alone.wait_recv()
            aside(1).wait_recv()

            @pl.when(k < forwarded)
            def _():
                for c in up(1):
                    c.start()

        @pl.when(jnp.logical_and(core == 0, jnp.logical_not(deputy)))
        def _():
            down(k).wait_recv()

            @pl.when(jnp.logical_and(jnp.logical_and(lead, k == near), jnp.logical_and(z > near, z <= most)))
            def _():
                pl.semaphore_signal(ready_sem, inc=1, device_id=at(z - near, 0), device_id_type=MESH)

        reaches_first = jnp.logical_and(lead, k == z)

        @pl.when(reaches_first)
        def _():
            @pl.when(early)
            def _():
                pass_on()
                for xx in range(1, chips):
                    project_out(xx)

            late_rates[0].wait_recv()
            pl.when(jnp.logical_and(relays, z < near // 2))(relay)
            rate_now[...] = late_rate[...].astype(F32)

        @pl.when(jnp.logical_not(reaches_first))
        def _():
            slab_rate(k)

        @pl.when(jnp.logical_or(k <= far, z <= alone_to))
        def _():
            attend(queries, k, False)

        return carry

    lax.fori_loop(1, received + 1, absorb, 0)

    @pl.when(guest)
    def _():
        answer.wait_recv()
        acc[...] = acc[...] + jnp.exp(-past[...]) * jnp.concatenate([far_got[...].astype(F32)] * 2, axis=0)

    @pl.when(jnp.logical_not(outset))
    def _():
        mixed[t] = join_heads(acc[...]).astype(BF16)

    @pl.when(jnp.logical_not(outset))
    def _():
        for d in sorted(range(1, chips), key=lambda d: -min(d, chips - d)):
            for c in range(2):
                p = 2 * lax.rem(x + d, chips) + c

                @pl.when(jnp.logical_or(z > 0, p != 0))
                def _():
                    mx_copy(p).start()

        @pl.when(jnp.logical_not(helper))
        def _():
            mx_copy(sibling).start()

    pl.when(jnp.logical_not(early))(pass_on)

    def serve():
        ask.wait_recv()
        split_heads(far_queries, far_in[...])
        other_acc[...] = jnp.zeros_like(other_acc)
        other_past[...] = jnp.zeros_like(other_past)

        def absorb_far(k, carry):
            reaches_first = jnp.logical_and(lead, k == z)

            @pl.when(reaches_first)
            def _():
                rate_now[...] = late_rate[...].astype(F32)

            @pl.when(jnp.logical_not(reaches_first))
            def _():
                slab_rate(k)

            attend(far_queries, k, False, other_acc, other_past)
            return carry

        lax.fori_loop(1, z + 1, absorb_far, 0)
        far_back[...] = join_heads(other_acc[...]).astype(BF16)
        answer.start()

    soon = z > reach // 2
    pl.when(jnp.logical_and(host, soon))(serve)
    pl.when(jnp.logical_and(relays, z >= near // 2))(relay)

    @pl.when(jnp.logical_not(jnp.logical_or(outset, early)))
    def _():
        for xx in range(1, chips):
            project_out(xx)

    pl.when(jnp.logical_and(host, jnp.logical_not(soon)))(serve)

    @pl.when(helper)
    def _():
        for c in back:
            c.wait_recv()
        split_heads(first_queries, first_q[...])
        late_rates[0].wait_recv()
        rate_now[...] = late_rate[...].astype(F32)
        attend(first_queries, 1, True, other_acc, other_past, 0)
        first_mixed[...] = join_heads(other_acc[...]).astype(BF16)
        for p in first_order:
            first_copy(p).start()
        mixed[0] = first_mixed[...]

    @pl.when(jnp.logical_not(outset))
    def _():
        project_out(0)

    handed = send(out, out, out_send, out_recv, z, sibling)

    @pl.when(helper)
    def _():
        pl.semaphore_wait(late_sem, 1)
        handed.start()
        handed.wait_send()

    @pl.when(outset)
    def _():
        handed.wait_recv()

    def left(ref, sem):
        send(ref, ref, sem, out_recv, z, sibling).wait_send()

    @pl.when(outset)
    def _():
        left(rate, lr_send.at[0])
        left(late_span, lr_send.at[1])

    @pl.when(helper)
    def _():
        borrowed.wait_send()
        alone.wait_send()
        if chips > 1:
            left(w_all.at[pl.ds(0, chips - 1)], w_send)
        if ntp > 2:
            left(mixed.at[pl.ds(0, ntp - 2)], first_send)

    carrier = jnp.logical_and(core == 1, jnp.logical_not(helper))
    for n in range(1, most + 1):

        @pl.when(jnp.logical_and(carrier, forwarded == n))
        def _():
            left(kv.at[pl.ds(0, n)], kv_send)

        @pl.when(
            jnp.logical_and(
                jnp.logical_and(core == 1, received == n), jnp.logical_not(jnp.logical_and(z == 1, t == 1))
            )
        )
        def _():
            left(kv.at[pl.ds(0, n), 0], down_send)

    @pl.when(jnp.logical_and(jnp.logical_and(core == 0, jnp.logical_not(outset)), forwarded > 0))
    def _():
        pl.when(deputy)(lambda: left(kv.at[0], kv_send))
        pl.when(jnp.logical_not(deputy))(lambda: left(kv.at[0, 0], kv_send))

    @pl.when(jnp.logical_not(jnp.logical_and(first, x == 0)))
    def _():
        left(w_all.at[pl.ds(0, ntp - 1)], w_send)

    @pl.when(z > 0)
    def _():
        left(mixed.at[pl.ds(0, ntp - 1)], mx_send)

    if ntp > 2:

        @pl.when(jnp.logical_and(first, t != 0))
        def _():
            left(mixed.at[pl.ds(0, ntp - 2)], mx_send)

    @pl.when(deputy)
    def _():
        left(w_all.at[pl.ds(0, chips)], lent_send)
        for c in back:
            c.wait_send()

    @pl.when(relays)
    def _():
        relayed.wait_send()

    @pl.when(guest)
    def _():
        ask.wait_send()

    @pl.when(host)
    def _():
        answer.wait_send()


def on_device(tokens, norm_gain, w_query, w_key, w_value, w_out, key_rate):
    nsp, ntp = lax.axis_size("sp"), lax.axis_size("tp")
    rows, d = tokens.shape
    width = w_query.shape[1]
    far = nsp // 2
    alone_to = min(far + SKIP, nsp - 1)
    most = max(alone_to, nsp - 1 - far)
    chips = ntp // 2
    dma = pltpu.SemaphoreType.DMA
    vmem = pltpu.VMEM
    return pl.pallas_call(
        functools.partial(layer, nsp, ntp, far, alone_to),
        out_shape=jax.ShapeDtypeStruct((rows, d), BF16),
        in_specs=[pl.BlockSpec(memory_space=pltpu.VMEM if i in (1, 6) else pltpu.HBM) for i in range(7)],
        out_specs=pl.BlockSpec(memory_space=pltpu.VMEM),
        scratch_shapes=[
            vmem((rows, d), BF16),
            vmem((d, width), BF16),
            vmem((d, width), BF16),
            vmem((d, width), BF16),
            vmem((width, d), BF16),
            vmem((most + 1, 2, 2 * SPAN + PAD, width), BF16),
            vmem((rows, d), BF16),
            vmem((rows, d), BF16),
            vmem((2 * rows, width), BF16),
            vmem((rows, width), BF16),
            vmem((2 * rows, width), BF16),
            vmem((rows, width), BF16),
            vmem((rows, width), BF16),
            vmem((2 * rows, width), BF16),
            vmem((rows, width), BF16),
            vmem((rows, width), BF16),
            vmem((2 * SPAN, 2 * SPAN), BF16),
            vmem((2, SPAN), F32),
            vmem((2, SPAN), BF16),
            vmem((min(nsp // 4, most), 2, SPAN), BF16),
            vmem((2 * rows, width), F32),
            vmem((2 * rows, SPAN), F32),
            vmem((2 * rows, width), F32),
            vmem((2 * rows, SPAN), F32),
            vmem((ntp, rows, width), BF16),
            vmem((rows, width), BF16),
            vmem((ntp, width, d), BF16),
            vmem((rows, d), F32),
            pltpu.SemaphoreType.REGULAR,
            pltpu.SemaphoreType.REGULAR,
            dma((5,)),
            dma,
            dma((most + 1, len(CHUNKS))),
            dma,
            dma,
            dma,
            dma((ntp,)),
            dma,
            dma,
            dma((ntp,)),
            dma,
            dma,
            dma((2,)),
            dma,
            dma,
            dma((2,)),
            dma((2,)),
            dma,
            dma,
            dma,
            dma,
            dma,
            dma,
        ],
        compiler_params=pltpu.CompilerParams(
            collective_id=0, has_side_effects=True, vmem_limit_bytes=55_650_000
        ),
    )(tokens, norm_gain.reshape(1, d), w_query, w_key, w_value, w_out, key_rate)


def solution(mesh):
    return jax.shard_map(
        on_device,
        mesh=mesh,
        in_specs=(
            P(("grp", "sp"), None),
            P(),
            P(None, "tp"),
            P(None, "tp"),
            P(None, "tp"),
            P("tp", None),
            P("tp", ("grp", "sp")),
        ),
        out_specs=P(("grp", "sp"), None),
        check_vma=False,
    )
```

```python
import functools

import jax
import jax.numpy as jnp
from jax import lax
from jax.experimental import pallas as pl
from jax.experimental.pallas import tpu as pltpu
from jax.sharding import PartitionSpec as P

HD = 64
SPAN = 128
PAD = 8
VAL = SPAN
CHUNKS = ((0, 96), (96, 80), (176, 88))

F32 = jnp.float32
BF16 = jnp.bfloat16
EPS = 1e-06
SKIP = 3
MESH = pl.DeviceIdType.MESH


def dot(a, b):
    return lax.dot_general(a, b, (((1,), (0,)), ((), ())), preferred_element_type=F32)


def dot_t(a, b):
    return lax.dot_general(a, b, (((1,), (1,)), ((), ())), preferred_element_type=F32)


def layer(
    nsp,
    ntp,
    far,
    alone_to,
    tokens_hbm,
    gain,
    w_query_hbm,
    w_key_hbm,
    w_value_hbm,
    w_out_hbm,
    rate,
    out,
    tokens,
    w_query,
    w_key,
    w_value,
    w_out,
    kv,
    normed,
    other_tokens,
    queries,
    first_q,
    first_queries,
    far_sent,
    far_in,
    far_queries,
    far_back,
    far_got,
    tri,
    rate_now,
    late_rate,
    late_span,
    acc,
    past,
    other_acc,
    other_past,
    mixed,
    first_mixed,
    w_all,
    total,
    late_sem,
    ready_sem,
    load,
    kv_send,
    kv_recv,
    down_send,
    w_send,
    lent_send,
    w_recv,
    mx_send,
    first_send,
    mx_recv,
    tok_send,
    tok_recv,
    lr_send,
    lr_recv,
    relay_send,
    h_send,
    h_recv,
    fq_send,
    fq_recv,
    fa_send,
    fa_recv,
    out_send,
    out_recv,
):
    z = lax.axis_index("sp")
    t = lax.axis_index("tp")
    chips = ntp // 2
    x, core = t // 2, lax.rem(t, 2)
    sibling = 2 * x + 1 - core
    reach = nsp - 1 - far
    most = max(alone_to, reach)
    near = min(nsp // 4, most)
    lead = t == 0
    first = z == 0
    last = z == nsp - 1
    outset = jnp.logical_and(first, lead)
    deputy = jnp.logical_and(z == 1, lead)
    helper = jnp.logical_and(first, t == 1)
    host = jnp.logical_and(z > alone_to - far, z <= reach)
    guest = z > alone_to

    bar = pltpu.get_barrier_semaphore()

    def at(zz, tt):
        return {"sp": zz, "tp": tt}

    def greet(zz, tt):
        pl.semaphore_signal(bar, inc=1, device_id=at(zz, tt), device_id_type=MESH)

    def send(src, dst, ss, rs, zz, tt):
        return pltpu.make_async_remote_copy(
            src_ref=src, dst_ref=dst, send_sem=ss, recv_sem=rs, device_id=at(zz, tt), device_id_type=MESH
        )

    loads = [
        pltpu.make_async_copy(a, b, load.at[i])
        for i, (a, b) in enumerate(
            (
                (tokens_hbm, tokens),
                (w_query_hbm, w_query),
                (w_key_hbm, w_key),
                (w_value_hbm, w_value),
                (w_out_hbm, w_out),
            )
        )
    ]

    @pl.when(jnp.logical_not(outset))
    def _():
        for c in loads:
            c.start()

    @pl.when(jnp.logical_and(z >= 1, core == 1))
    def _():
        greet(z - 1, t)

    for p in range(ntp):

        @pl.when(jnp.logical_and(t != 0, t != p))
        def _():
            greet(z, p)

    @pl.when(host)
    def _():
        greet(z + far, t)

    @pl.when(jnp.logical_and(jnp.logical_and(z >= 1, z <= near), lead))
    def _():
        greet(0, 0)

    @pl.when(jnp.logical_and(first, t != 0))
    def _():
        greet(1, 0)

    @pl.when(deputy)
    def _():
        greet(0, 1)

    one = lambda flag: jnp.where(flag, 1, 0)
    expected = (
        one(jnp.logical_and(jnp.logical_not(last), core == 1))
        + jnp.where(lead, ntp - 1, ntp - 2)
        + one(guest)
        + one(outset) * near
        + one(deputy) * (ntp - 1)
        + one(helper)
    )

    late_rates = [send(rate, late_rate, lr_send.at[0], lr_recv, 0, 1)] + [
        send(rate, late_rate, lr_send.at[1], lr_recv, i, 0) for i in range(1, near + 1)
    ]

    @pl.when(outset)
    def _():
        pl.semaphore_wait(bar, expected)
        for c in late_rates:
            c.start()

    @pl.when(jnp.logical_not(outset))
    def _():
        row = lax.broadcasted_iota(jnp.int32, (2 * SPAN, 2 * SPAN), 0)
        col = lax.broadcasted_iota(jnp.int32, (2 * SPAN, 2 * SPAN), 1)
        later = jnp.logical_or(col >= SPAN, lax.rem(row, SPAN) >= col)
        tri[...] = jnp.where(later, 1.0, 0.0).astype(BF16)

    def split_heads(dst, q):
        lane = lax.broadcasted_iota(jnp.int32, (SPAN, 2 * HD), 1)
        qf = q.astype(F32)
        dst[:SPAN] = jnp.where(lane < HD, qf, 0.0).astype(BF16)
        dst[SPAN:] = jnp.where(lane >= HD, qf, 0.0).astype(BF16)

    def join_heads(a):
        lane = lax.broadcasted_iota(jnp.int32, (SPAN, 2 * HD), 1)
        return jnp.where(lane < HD, a[:SPAN], a[SPAN:])

    def project_queries(src, wait):
        wait(0)
        xs = src[...].astype(F32)
        scale = lax.rsqrt(jnp.mean(xs * xs, axis=-1, keepdims=True) + EPS)
        normed[...] = (xs * scale * gain[...]).astype(BF16)
        wait(1)
        return dot(normed[...], w_query[...]).astype(BF16) * HD ** (-0.5)

    def project_slab(slot, wait):
        wait(2)
        kv[slot, core, pl.ds(0, SPAN)] = dot(normed[...], w_key[...]).astype(BF16)
        wait(3)
        kv[slot, core, pl.ds(VAL, SPAN)] = dot(normed[...], w_value[...]).astype(BF16)
        kv[slot, core, pl.ds(2 * SPAN, PAD)] = jnp.concatenate(
            [rate[...].astype(F32), jnp.zeros((PAD - 2, SPAN), F32)], axis=0
        ).astype(BF16)

    def attend(q_ref, slot, diagonal, acc=acc, past=past, part=core):
        s = dot_t(q_ref[...], kv[slot, part, pl.ds(0, SPAN)])
        s = jnp.concatenate([s[:SPAN] + rate_now[0:1], s[SPAN:] + rate_now[1:2]], axis=0)
        soft = jnp.maximum(s, 0.0) + jnp.log(1.0 + jnp.exp(-jnp.abs(s)))
        if diagonal:
            r = lax.rem(lax.broadcasted_iota(jnp.int32, (2 * SPAN, SPAN), 0), SPAN)
            c = lax.broadcasted_iota(jnp.int32, (2 * SPAN, SPAN), 1)
            seen = c < r
            soft = jnp.where(seen, soft, 0.0)
        high = soft.astype(BF16)
        low = (soft - high.astype(F32)).astype(BF16)
        sums = dot(jnp.concatenate([high, low], axis=1), tri[...])
        weight = jnp.exp(s - sums[:, :SPAN])
        if diagonal:
            weight = jnp.where(seen, weight, 0.0)
        got = dot(weight.astype(BF16), kv[slot, part, pl.ds(VAL, SPAN)])
        if diagonal:
            acc[...] = got
            past[...] = sums[:, SPAN:]
        else:
            acc[...] = acc[...] + jnp.exp(-past[...]) * got
            past[...] = past[...] + sums[:, SPAN:]

    def slab_rate(slot):
        rate_now[...] = kv[slot, core, pl.ds(2 * SPAN, PAD)][:2].astype(F32)

    ask = send(far_sent, far_in, fq_send, fq_recv, z - far, t)
    answer = send(far_back, far_got, fa_send, fa_recv, z + far, t)

    @pl.when(jnp.logical_not(outset))
    def _():
        q = project_queries(tokens, lambda i: loads[i].wait())
        far_sent[...] = q
        split_heads(queries, q)

        @pl.when(jnp.logical_not(guest))
        def _():
            project_slab(0, lambda i: loads[i].wait())

        pl.semaphore_wait(bar, expected)

        @pl.when(guest)
        def _():
            ask.start()
            project_slab(0, lambda i: loads[i].wait())

        slab_rate(0)
        loads[4].wait()

    borrowed = send(tokens, other_tokens, tok_send, tok_recv, 1, 0)

    def w_copy(src, slot, sem, zz, tt):
        return send(src, w_all.at[slot], sem, w_recv.at[slot], zz, tt)

    def across(d):
        return 2 * lax.rem(x + d, chips) + core

    directs = [w_copy(w_out, t, w_send, z, across(d)) for d in range(1, chips)]
    to_sibling = w_copy(w_out, t, w_send, z, sibling)
    passed = [w_copy(w_all.at[across(d)], across(d), w_send, z, sibling) for d in range(1, chips)]
    lent = [w_copy(w_out, 0, lent_send, 0, p) for p in [1] + list(range(2, ntp, 2))]
    to_helper = w_copy(w_out, t, w_send, 0, 1)

    def up(k):
        return [
            send(kv.at[k, :, pl.ds(a, n)], kv.at[k + 1, :, pl.ds(a, n)], kv_send, kv_recv.at[k + 1, c], z + 1, t)
            for c, (a, n) in enumerate(CHUNKS)
        ]

    def down(k):
        return send(kv.at[k, 0], kv.at[k, 0], down_send, kv_recv.at[k, 0], z, sibling)

    def aside(k):
        return send(kv.at[k, 0], kv.at[k, 0], kv_send, kv_recv.at[k, 0], z, sibling)

    alone = send(kv.at[0, 1], kv.at[1, 1], kv_send, kv_recv.at[1, 1], 1, 1)
    back = [
        send(kv.at[1, 0], kv.at[1, 0], h_send.at[0], h_recv.at[0], 0, 1),
        send(first_q, first_q, h_send.at[1], h_recv.at[1], 0, 1),
    ]

    def mx_copy(p):
        return send(mixed.at[t], mixed.at[t], mx_send, mx_recv.at[t], z, p)

    def first_copy(p):
        return send(first_mixed, mixed.at[0], first_send, mx_recv.at[0], 0, p)

    first_order = list(range(4, min(6, ntp))) + [p for p in range(2, ntp) if p not in (4, 5)]

    def needed(zz):
        return jnp.where(zz <= most, zz, far)

    received = needed(z)
    forwarded = jnp.where(last, 0, needed(z + 1))

    @pl.when(helper)
    def _():
        borrowed.start()

    @pl.when(helper)
    def _():
        alone.start()

    @pl.when(jnp.logical_and(jnp.logical_and(core == 0, jnp.logical_not(outset)), forwarded > 0))
    def _():
        aside(0).start()

    for p in range(1, ntp):

        @pl.when(jnp.logical_and(lead, z > 0) if p > 1 else lead)
        def _():
            pl.semaphore_signal(late_sem, inc=1, device_id=at(z, p), device_id_type=MESH)

    @pl.when(jnp.logical_not(outset))
    def _():
        for d in range(1, chips):

            @pl.when(across(d) != 0)
            def _():
                directs[d - 1].start()

        @pl.when(sibling != 0)
        def _():
            to_sibling.start()

    @pl.when(deputy)
    def _():
        for c in lent:
            c.start()

    @pl.when(jnp.logical_and(first, jnp.logical_and(core == 0, t != 0)))
    def _():
        to_helper.start()

    def to_lead():
        pl.semaphore_wait(late_sem, 1)
        for d in range(1, chips):

            @pl.when(across(d) == 0)
            def _():
                directs[d - 1].start()

        @pl.when(sibling == 0)
        def _():
            to_sibling.start()

    @pl.when(jnp.logical_and(z > 0, t != 0))
    def _():
        to_lead()

    @pl.when(jnp.logical_not(outset))
    def _():
        w_all[t] = w_out[...]

    @pl.when(deputy)
    def _():
        borrowed.wait_recv()
        first_q[...] = project_queries(other_tokens, lambda i: None)
        project_slab(1, lambda i: None)
        aside(1).start()
        for c in back:
            c.start()

    def wait_w(slot):
        w_copy(w_out, slot, w_send, z, t).wait_recv()

    def wait_mixed(slot):
        send(mixed.at[slot], mixed.at[slot], mx_send, mx_recv.at[slot], z, t).wait_recv()

    def project_out(xx):
        for slot in (2 * xx, 2 * xx + 1):
            pl.when(core != slot % 2)(functools.partial(wait_w, slot))
            pl.when(jnp.logical_and(t != slot, jnp.logical_not(helper)) if slot == 0 else t != slot)(
                functools.partial(wait_mixed, slot)
            )
        pair = jnp.concatenate([mixed[2 * xx], mixed[2 * xx + 1]], axis=1)
        rows = jnp.concatenate([w_all[2 * xx], w_all[2 * xx + 1]], axis=0)
        got = dot(pair, rows)
        if xx == 1 and chips > 1:
            total[...] = got
        elif xx > 0:
            total[...] = total[...] + got
        else:
            out[...] = (total[...] + got if chips > 1 else got).astype(BF16)

    def pass_on():
        for d in range(1, chips):

            @pl.when(jnp.logical_not(outset))
            def _():
                w_copy(w_out, across(d), w_send, z, t).wait_recv()

            @pl.when(jnp.logical_not(jnp.logical_and(first, x == 0)))
            def _():
                passed[d - 1].start()

    early = jnp.logical_and(lead, jnp.logical_and(z >= 1, z <= reach // 2))

    relays = jnp.logical_and(lead, jnp.logical_and(z >= 1, z <= most - near))
    relayed = send(late_rate, late_rate, relay_send, lr_recv, z + near, 0)

    def relay():
        pl.semaphore_wait(ready_sem, 1)
        relayed.start()

    @pl.when(jnp.logical_and(jnp.logical_and(core == 1, forwarded > 0), jnp.logical_not(helper)))
    def _():
        aside(0).wait_recv()
        for c in up(0):
            c.start()

    @pl.when(jnp.logical_not(outset))
    def _():
        attend(queries, 0, True)

    def absorb(k, carry):
        beside = jnp.logical_and(z == 1, t == 1)

        @pl.when(jnp.logical_and(core == 1, jnp.logical_not(beside)))
        def _():
            for c in range(len(CHUNKS)):
                up(k - 1)[c].wait_recv()

                @pl.when(k < forwarded)
                def _():
                    up(k)[c].start()

            down(k).start()

        @pl.when(beside)
        def _():
            alone.wait_recv()
            aside(1).wait_recv()

            @pl.when(k < forwarded)
            def _():
                for c in up(1):
                    c.start()

        @pl.when(jnp.logical_and(core == 0, jnp.logical_not(deputy)))
        def _():
            down(k).wait_recv()

            @pl.when(jnp.logical_and(jnp.logical_and(lead, k == near), jnp.logical_and(z > near, z <= most)))
            def _():
                pl.semaphore_signal(ready_sem, inc=1, device_id=at(z - near, 0), device_id_type=MESH)

        reaches_first = jnp.logical_and(lead, k == z)

        @pl.when(reaches_first)
        def _():
            @pl.when(early)
            def _():
                pass_on()
                for xx in range(1, chips):
                    project_out(xx)

            late_rates[0].wait_recv()
            pl.when(jnp.logical_and(relays, z < near // 2))(relay)
            rate_now[...] = late_rate[...].astype(F32)

        @pl.when(jnp.logical_not(reaches_first))
        def _():
            slab_rate(k)

        @pl.when(jnp.logical_or(k <= far, z <= alone_to))
        def _():
            attend(queries, k, False)

        return carry

    lax.fori_loop(1, received + 1, absorb, 0)

    @pl.when(guest)
    def _():
        answer.wait_recv()
        acc[...] = acc[...] + jnp.exp(-past[...]) * jnp.concatenate([far_got[...].astype(F32)] * 2, axis=0)

    @pl.when(jnp.logical_not(outset))
    def _():
        mixed[t] = join_heads(acc[...]).astype(BF16)

    @pl.when(jnp.logical_not(outset))
    def _():
        for d in sorted(range(1, chips), key=lambda d: -min(d, chips - d)):
            for c in range(2):
                p = 2 * lax.rem(x + d, chips) + c

                @pl.when(jnp.logical_or(z > 0, p != 0))
                def _():
                    mx_copy(p).start()

        @pl.when(jnp.logical_not(helper))
        def _():
            mx_copy(sibling).start()

    pl.when(jnp.logical_not(early))(pass_on)

    def serve():
        ask.wait_recv()
        split_heads(far_queries, far_in[...])
        other_acc[...] = jnp.zeros_like(other_acc)
        other_past[...] = jnp.zeros_like(other_past)

        def absorb_far(k, carry):
            reaches_first = jnp.logical_and(lead, k == z)

            @pl.when(reaches_first)
            def _():
                rate_now[...] = late_rate[...].astype(F32)

            @pl.when(jnp.logical_not(reaches_first))
            def _():
                slab_rate(k)

            attend(far_queries, k, False, other_acc, other_past)
            return carry

        lax.fori_loop(1, z + 1, absorb_far, 0)
        far_back[...] = join_heads(other_acc[...]).astype(BF16)
        answer.start()

    soon = z > reach // 2
    pl.when(jnp.logical_and(host, soon))(serve)
    pl.when(jnp.logical_and(relays, z >= near // 2))(relay)

    @pl.when(jnp.logical_not(jnp.logical_or(outset, early)))
    def _():
        for xx in range(1, chips):
            project_out(xx)

    pl.when(jnp.logical_and(host, jnp.logical_not(soon)))(serve)

    @pl.when(helper)
    def _():
        for c in back:
            c.wait_recv()
        split_heads(first_queries, first_q[...])
        late_rates[0].wait_recv()
        rate_now[...] = late_rate[...].astype(F32)
        attend(first_queries, 1, True, other_acc, other_past, 0)
        first_mixed[...] = join_heads(other_acc[...]).astype(BF16)
        for p in first_order:
            first_copy(p).start()
        mixed[0] = first_mixed[...]

    @pl.when(jnp.logical_not(outset))
    def _():
        project_out(0)

    handed = send(out, out, out_send, out_recv, z, sibling)

    @pl.when(helper)
    def _():
        pl.semaphore_wait(late_sem, 1)
        handed.start()
        handed.wait_send()

    @pl.when(outset)
    def _():
        handed.wait_recv()

    def left(ref, sem):
        send(ref, ref, sem, out_recv, z, sibling).wait_send()

    @pl.when(outset)
    def _():
        left(rate, lr_send.at[0])
        left(late_span, lr_send.at[1])

    @pl.when(helper)
    def _():
        borrowed.wait_send()
        alone.wait_send()
        if chips > 1:
            left(w_all.at[pl.ds(0, chips - 1)], w_send)
        if ntp > 2:
            left(mixed.at[pl.ds(0, ntp - 2)], first_send)

    carrier = jnp.logical_and(core == 1, jnp.logical_not(helper))
    for n in range(1, most + 1):

        @pl.when(jnp.logical_and(carrier, forwarded == n))
        def _():
            left(kv.at[pl.ds(0, n)], kv_send)

        @pl.when(
            jnp.logical_and(
                jnp.logical_and(core == 1, received == n), jnp.logical_not(jnp.logical_and(z == 1, t == 1))
            )
        )
        def _():
            left(kv.at[pl.ds(0, n), 0], down_send)

    @pl.when(jnp.logical_and(jnp.logical_and(core == 0, jnp.logical_not(outset)), forwarded > 0))
    def _():
        pl.when(deputy)(lambda: left(kv.at[0], kv_send))
        pl.when(jnp.logical_not(deputy))(lambda: left(kv.at[0, 0], kv_send))

    @pl.when(jnp.logical_not(jnp.logical_and(first, x == 0)))
    def _():
        left(w_all.at[pl.ds(0, ntp - 1)], w_send)

    @pl.when(z > 0)
    def _():
        left(mixed.at[pl.ds(0, ntp - 1)], mx_send)

    if ntp > 2:

        @pl.when(jnp.logical_and(first, t != 0))
        def _():
            left(mixed.at[pl.ds(0, ntp - 2)], mx_send)

    @pl.when(deputy)
    def _():
        left(w_all.at[pl.ds(0, chips)], lent_send)
        for c in back:
            c.wait_send()

    @pl.when(relays)
    def _():
        relayed.wait_send()

    @pl.when(guest)
    def _():
        ask.wait_send()

    @pl.when(host)
    def _():
        answer.wait_send()


def on_device(tokens, norm_gain, w_query, w_key, w_value, w_out, key_rate):
    nsp, ntp = lax.axis_size("sp"), lax.axis_size("tp")
    rows, d = tokens.shape
    width = w_query.shape[1]
    far = nsp // 2
    alone_to = min(far + SKIP, nsp - 1)
    most = max(alone_to, nsp - 1 - far)
    chips = ntp // 2
    dma = pltpu.SemaphoreType.DMA
    vmem = pltpu.VMEM
    return pl.pallas_call(
        functools.partial(layer, nsp, ntp, far, alone_to),
        out_shape=jax.ShapeDtypeStruct((rows, d), BF16),
        in_specs=[pl.BlockSpec(memory_space=pltpu.VMEM if i in (1, 6) else pltpu.HBM) for i in range(7)],
        out_specs=pl.BlockSpec(memory_space=pltpu.VMEM),
        scratch_shapes=[
            vmem((rows, d), BF16),
            vmem((d, width), BF16),
            vmem((d, width), BF16),
            vmem((d, width), BF16),
            vmem((width, d), BF16),
            vmem((most + 1, 2, 2 * SPAN + PAD, width), BF16),
            vmem((rows, d), BF16),
            vmem((rows, d), BF16),
            vmem((2 * rows, width), BF16),
            vmem((rows, width), BF16),
            vmem((2 * rows, width), BF16),
            vmem((rows, width), BF16),
            vmem((rows, width), BF16),
            vmem((2 * rows, width), BF16),
            vmem((rows, width), BF16),
            vmem((rows, width), BF16),
            vmem((2 * SPAN, 2 * SPAN), BF16),
            vmem((2, SPAN), F32),
            vmem((2, SPAN), BF16),
            vmem((min(nsp // 4, most), 2, SPAN), BF16),
            vmem((2 * rows, width), F32),
            vmem((2 * rows, SPAN), F32),
            vmem((2 * rows, width), F32),
            vmem((2 * rows, SPAN), F32),
            vmem((ntp, rows, width), BF16),
            vmem((rows, width), BF16),
            vmem((ntp, width, d), BF16),
            vmem((rows, d), F32),
            pltpu.SemaphoreType.REGULAR,
            pltpu.SemaphoreType.REGULAR,
            dma((5,)),
            dma,
            dma((most + 1, len(CHUNKS))),
            dma,
            dma,
            dma,
            dma((ntp,)),
            dma,
            dma,
            dma((ntp,)),
            dma,
            dma,
            dma((2,)),
            dma,
            dma,
            dma((2,)),
            dma((2,)),
            dma,
            dma,
            dma,
            dma,
            dma,
            dma,
        ],
        compiler_params=pltpu.CompilerParams(
            collective_id=0, has_side_effects=True, vmem_limit_bytes=55_650_000
        ),
    )(tokens, norm_gain.reshape(1, d), w_query, w_key, w_value, w_out, key_rate)


def solution(mesh):
    return jax.shard_map(
        on_device,
        mesh=mesh,
        in_specs=(
            P(("grp", "sp"), None),
            P(),
            P(None, "tp"),
            P(None, "tp"),
            P(None, "tp"),
            P("tp", None),
            P("tp", ("grp", "sp")),
        ),
        out_specs=P(("grp", "sp"), None),
        check_vma=False,
    )
```
